256 devices in a mesh: sp: 32 (over z, x), tp: 8 (over y, core).
Axes of the slice: x: 4, y: 4, z: 8, core: 2. Of those that a mesh axis runs over, the one named last changes fastest.
Arguments:
- resid: bfloat16 [12288, 2048], P('sp'), may hold values from -6 to 6
- cotangent: bfloat16 [12288, 2048], P('sp'), may hold values from -0.59765625 to 0.59765625
- routes: int32 [12288, 2], P('sp'), may hold values from 0 to 31, all different within a row; in each aligned block of 384 rows (0 to 383, 384 to 767, ...) at most 48 rows name the same one
- route_weight: float32 [12288, 2], P('sp'), may hold values from 0.3 to 2.2
- w_gate: bfloat16 [32, 2048, 1024], P('sp', None, 'tp'), may hold values from -0.125 to 0.125
- w_up: bfloat16 [32, 2048, 1024], P('sp', None, 'tp'), may hold values from -0.125 to 0.125
- w_down: bfloat16 [32, 1024, 2048], P('sp', 'tp'), may hold values from -0.1875 to 0.1875
- out_proj: bfloat16 [2048, 2816], P(None, 'tp'), may hold values from -0.109375 to 0.109375
- gate_pre: bfloat16 [12288, 2816], P('sp', 'tp'), may hold values from -8 to 8
- log_decay: float32 [12288, 2816], P('sp', 'tp'), may hold values from -1 to 0
- state_before: float32 [12288, 2816], P('sp', 'tp'), may hold values from -6 to 6
- step_input: bfloat16 [12288, 2816], P('sp', 'tp'), may hold values from -6 to 6
Outputs:
- grad_gate: float32 [32, 2048, 1024], P('sp', None, 'tp')
- grad_up: float32 [32, 2048, 1024], P('sp', None, 'tp')
- grad_down: float32 [32, 1024, 2048], P('sp', 'tp')
- grad_proj: float32 [2048, 2816], P('sp', 'tp')
- grad_gate_pre: bfloat16 [12288, 2816], P('sp', 'tp')
- grad_step_input: float32 [12288, 2816], P('sp', 'tp')
- grad_log_decay: float32 [12288, 2816], P('sp', 'tp')
The draws below stay inside these ranges and needn't reach their ends.
Inputs may be any that keep to these rules, and one draw needn't show every extreme that they name: `routes`: each row names 2 different experts. In the rows of one device no expert is named more than 48 times; some expert is named exactly 48 times in the rows of some devices.
All inputs are finite; a program needn't handle non-finite values.
Results may differ from the reference program's by a relative error of at most 0.02.
Values may be sent and summed in bfloat16 or wider, within the bound.
A program may use at most 128 MiB of HBM per device.

```python
import math
import jax
import jax.numpy as jnp
import numpy as np
from jax import lax

D = 2048
HEADS = 32
HEAD_DIM = 88
FE = 1024
TOP = 2
TOK_DEV = 384
STATE_CHANNELS = 2816
SEQUENCE_TOKENS = 12288
EXPERTS = 32
CAP = 48
N_SP = 32
N_TP = 8


def draw_log_decay(key, part):
    random_subkeys = jax.random.split(jax.random.fold_in(key, 17), 7)
    head_fast_prob = 0.5
    is_fast = jax.random.bernoulli(random_subkeys[0], head_fast_prob, (HEADS,))
    is_fast = jnp.repeat(is_fast, HEAD_DIM)
    slow_rate = jnp.exp(jax.random.uniform(random_subkeys[1], (STATE_CHANNELS,), jnp.float32, -0.69, 0.0)) * (0.15 / SEQUENCE_TOKENS)
    fast_rate = jax.random.uniform(random_subkeys[2], (STATE_CHANNELS,), jnp.float32, 1.0 / 50.0, 1.0 / 30.0)
    decay_rates = jnp.where(is_fast, fast_rate, slow_rate)
    jagged_level = jnp.exp(jax.random.uniform(random_subkeys[3], (SEQUENCE_TOKENS, STATE_CHANNELS), jnp.float32, -0.7, 0.7))
    block_multiplier = jnp.exp(jax.random.uniform(random_subkeys[4], (SEQUENCE_TOKENS // TOK_DEV, 1), jnp.float32, -0.69, 0.69))
    block_multiplier = jnp.repeat(block_multiplier, TOK_DEV, axis=0)
    spike_location = jax.random.randint(random_subkeys[5], (3,), 0, SEQUENCE_TOKENS)
    token_position = jnp.arange(SEQUENCE_TOKENS, dtype=jnp.int32)
    spike_flag = jnp.any(token_position[:, None] == spike_location[None, :], axis=1)
    spike_penalty = jax.random.uniform(random_subkeys[6], (SEQUENCE_TOKENS, STATE_CHANNELS), jnp.float32, 0.22, 0.69)
    return -(decay_rates[None, :] * jagged_level * block_multiplier) - jnp.where(spike_flag[:, None], spike_penalty, 0.0)


def with_spikes(drawn, own_key, source, target, shards_of, factor):
    def block_of(axis_at):
        return (jnp.arange(drawn.shape[axis_at]) // (drawn.shape[axis_at] // shards_of)).reshape((-1,) + (1,) * (drawn.ndim - 1 - axis_at))

    one_side = jax.random.permutation(own_key, shards_of)[block_of(target)]
    far = (block_of(target) + shards_of // 2) % shards_of
    return jnp.where((block_of(source) == one_side) | (block_of(source) == far), factor * drawn, drawn)


def steps_of(stream_key, extent, cuts, least, high):
    level = 1.0
    for dim, blocks in cuts:
        heights = jax.random.uniform(jax.random.fold_in(jax.random.fold_in(stream_key, 6), dim), (blocks,), jnp.float32, least / len(cuts), high / len(cuts))
        level = level * jnp.repeat(jnp.exp(heights), extent[dim] // blocks).reshape((-1,) + (1,) * (len(extent) - 1 - dim))
    return level


def shared_out(key, own, number, rows, number_of, top, bound, skew):
    order = jax.random.permutation(key, number_of)
    crowded, usual = portions_of(number_of, rows * top, bound, skew, True), portions_of(number_of, rows * top, bound, skew, False)
    places = jnp.arange(number_of)

    def named(tallies, turn):
        used = int((tallies > 0).sum())
        fixed = max(1, used // 4)
        moved = fixed + (places - fixed + turn * (used - fixed)) % max(1, number_of - fixed)
        return jnp.zeros((number_of,), jnp.int32).at[order[jnp.where(places < fixed, places, moved)]].set(jnp.asarray(tallies, jnp.int32))

    tallies = jnp.where(number % 4 == 0, named(crowded, number // 4), named(usual, number - number // 4 - 1))
    mixed = jax.random.permutation(jax.random.fold_in(own, 3), number_of)
    donor, taker = mixed[0:number_of // 2 * 2:2], mixed[1:number_of // 2 * 2:2]
    margin = jnp.minimum(tallies[donor] - 1, bound - tallies[taker]) // 2
    margin = jnp.where((donor == order[0]) | (taker == order[0]) | (tallies[taker] == 0), 0, jnp.maximum(margin, 0))
    moved = jax.random.randint(jax.random.fold_in(own, 4), (number_of // 2,), 0, 1 << 20) % (margin + 1)
    tallies = tallies.at[donor].add(-moved).at[taker].add(moved)
    items = jnp.searchsorted(jnp.cumsum(tallies), jnp.arange(rows * top), side="right").astype(jnp.int32)
    grid = items.reshape(top, rows).T
    grid = grid[jax.random.permutation(jax.random.fold_in(own, 1), rows)]
    turn = jax.random.randint(jax.random.fold_in(own, 2), (rows, 1), 0, top)
    return jnp.take_along_axis(grid, (jnp.arange(top)[None, :] + turn) % top, axis=1)


def portions_of(number_of, total, bound, skew, full):
    loads = [(1 << 20) // math.isqrt(standing ** skew) + 1 for standing in range(1, number_of + 1)]
    largest = bound if full else min(bound, max(-(-total // number_of), total * loads[0] // sum(loads)))
    least = 1 if total - largest >= number_of - 1 else 0
    counts, spare = [largest] + [least] * (number_of - 1), total - largest - least * (number_of - 1)
    while spare > 0:
        free = [i for i in range(1, number_of) if counts[i] < largest] or [i for i in range(1, number_of) if counts[i] < bound]
        mass, budget = sum([loads[i] for i in free]), spare
        for i in free:
            more = min(bound - counts[i], max(1, budget * loads[i] // mass), spare)
            counts[i] = counts[i] + more
            spare = spare - more
    return np.array(counts)


def centred(key, extent, width, bound, pieces=(), held_as=jnp.bfloat16):
    entries = jax.random.normal(key, extent, jnp.float32) * width
    if len(pieces) > 0:
        entries = steps_of(key, extent, pieces, -0.22, 0.18) * entries
    return jnp.clip(entries, min=-bound, max=bound).astype(held_as)


def heavy_noise(own_key, extent, width, limit, pieces, heavy, held_as=jnp.bfloat16):
    result = width * jax.random.normal(own_key, extent, jnp.float32)
    if pieces:
        result = result * steps_of(own_key, extent, pieces, -0.22, 0.18)
    return jnp.clip(with_spikes(result, jax.random.fold_in(own_key, 3), *heavy), -limit, limit).astype(held_as)


def setup_inputs(seed: int = 0) -> dict:
    splits = jax.random.split(jax.random.key(seed), 13)
    resid = centred(splits[0], (SEQUENCE_TOKENS, D), 1.0, 6.0, ((0, 32),))
    cotangent = heavy_noise(splits[1], (SEQUENCE_TOKENS, D), 0.1, 0.59765625, ((0, 32),), (0, 1, 32, 2.75))
    routes_keys = jax.random.split(jax.random.fold_in(splits[2], 1), SEQUENCE_TOKENS // TOK_DEV)
    routes_turns = jax.random.permutation(jax.random.fold_in(splits[2], 3), SEQUENCE_TOKENS // TOK_DEV)
    routes = jax.vmap(lambda own, number: shared_out(jax.random.fold_in(splits[2], 2), own, number, TOK_DEV, EXPERTS, TOP, CAP, 2))(routes_keys, routes_turns).reshape((SEQUENCE_TOKENS, TOP))
    route_weight = jnp.clip(jnp.exp(math.log(2.2) - 1.9924301 * jax.random.uniform(splits[3], (SEQUENCE_TOKENS, TOP), jnp.float32) ** steps_of(splits[3], (SEQUENCE_TOKENS, TOP), ((0, 32),), -0.2, 0.2)), 0.3, 2.2)
    w_gate = centred(splits[4], (EXPERTS, D, FE), D ** -0.5, 0.125, ((0, 32), (2, 8)))
    w_up = centred(splits[5], (EXPERTS, D, FE), D ** -0.5, 0.125, ((0, 32), (2, 8)))
    w_down = centred(splits[6], (EXPERTS, FE, D), FE ** -0.5, 0.1875, ((0, 32), (1, 8)))
    out_proj = centred(splits[7], (D, STATE_CHANNELS), STATE_CHANNELS ** -0.5, 0.109375, ((1, 8),))
    gate_pre = centred(splits[8], (SEQUENCE_TOKENS, STATE_CHANNELS), 1.5, 8.0, ((0, 32), (1, 8)))
    log_decay = draw_log_decay(jax.random.fold_in(splits[12], 71), 0)
    state_before = centred(splits[10], (SEQUENCE_TOKENS, STATE_CHANNELS), 1.0, 6.0, ((0, 32), (1, 8)), jnp.float32)
    step_input = centred(splits[11], (SEQUENCE_TOKENS, STATE_CHANNELS), 1.0, 6.0, ((0, 32), (1, 8)))
    return {"resid": resid, "cotangent": cotangent, "routes": routes, "route_weight": route_weight, "w_gate": w_gate, "w_up": w_up, "w_down": w_down, "out_proj": out_proj, "gate_pre": gate_pre, "log_decay": log_decay, "state_before": state_before, "step_input": step_input}


def slot_table(routes, route_weight):
    flat_ids = routes.reshape(N_SP, TOK_DEV * TOP)
    onehot = (flat_ids[:, :, None] == jnp.arange(EXPERTS, dtype=jnp.int32)[None, None, :]).astype(jnp.int32)
    ranking = lax.optimization_barrier(jnp.sum((jnp.cumsum(onehot, axis=1) - onehot) * onehot, axis=2)).reshape(-1)
    expert_ids = routes.reshape(-1)
    token_ids = jnp.arange(SEQUENCE_TOKENS * TOP, dtype=jnp.int32) // TOP
    block_ids = token_ids // TOK_DEV
    slot_token = jnp.full((EXPERTS, N_SP, CAP), SEQUENCE_TOKENS, jnp.int32).at[expert_ids, block_ids, ranking].set(token_ids)
    slot_weight = jnp.zeros((EXPERTS, N_SP, CAP), jnp.float32).at[expert_ids, block_ids, ranking].set(route_weight.reshape(-1))
    return (slot_token, slot_weight)

def one_expert(operands):
    token_ids, weights, resid_pad, cot_pad, gate_w, up_w, down_w = operands
    in_rows = resid_pad[token_ids]
    cot_rows = (weights[:, None] * cot_pad[token_ids].astype(jnp.float32)).astype(jnp.bfloat16)
    gate_act = jnp.dot(in_rows, gate_w, preferred_element_type=jnp.float32)
    up_act = jnp.dot(in_rows, up_w, preferred_element_type=jnp.float32)
    sigmoid_a = jax.nn.sigmoid(gate_act)
    hidden = (jax.nn.silu(gate_act) * up_act).astype(jnp.bfloat16)
    grad_down = jnp.dot(hidden.T, cot_rows, preferred_element_type=jnp.float32)
    d_hidden = jnp.dot(cot_rows, down_w.T, preferred_element_type=jnp.float32)
    slope = sigmoid_a * (1.0 + gate_act * (1.0 - sigmoid_a))
    d_gate_act = (d_hidden * up_act * slope).astype(jnp.bfloat16)
    d_up_act = (d_hidden * jax.nn.silu(gate_act)).astype(jnp.bfloat16)
    grad_gate = jnp.dot(in_rows.T, d_gate_act, preferred_element_type=jnp.float32)
    grad_up = jnp.dot(in_rows.T, d_up_act, preferred_element_type=jnp.float32)
    row_count = in_rows.shape[0]
    group = FE // N_TP
    parts = jnp.einsum('rpf,dpf->prd', d_gate_act.reshape(row_count, N_TP, group).astype(jnp.float32), gate_w.reshape(D, N_TP, group).astype(jnp.float32))
    parts = parts + jnp.einsum('rpf,dpf->prd', d_up_act.reshape(row_count, N_TP, group).astype(jnp.float32), up_w.reshape(D, N_TP, group).astype(jnp.float32))
    rounded = lax.optimization_barrier(parts.astype(jnp.bfloat16))
    expert_grad = lax.optimization_barrier(jnp.sum(rounded.astype(jnp.float32), axis=0)).astype(jnp.bfloat16)
    return (grad_gate, grad_up, grad_down, expert_grad)

def reverse_link(former, latter):
    return (former[0] * latter[0], latter[0] * former[1] + latter[1])

def reference(resid, cotangent, routes, route_weight, w_gate, w_up, w_down, out_proj, gate_pre, log_decay, state_before, step_input):
    slot_token, slot_weight = slot_table(routes, route_weight)
    resid_pad = jnp.concatenate([resid, jnp.zeros((1, D), jnp.bfloat16)], axis=0)
    cot_pad = jnp.concatenate([cotangent, jnp.zeros((1, D), jnp.bfloat16)], axis=0)

    def per_expert(operands):
        token_ids, weights, gate_w, up_w, down_w = operands
        return one_expert((token_ids.reshape(-1), weights.reshape(-1), resid_pad, cot_pad, gate_w, up_w, down_w))
    grad_gate, grad_up, grad_down, expert_grad = lax.map(per_expert, (slot_token, slot_weight, w_gate, w_up, w_down))
    routed = jnp.zeros((SEQUENCE_TOKENS + 1, D), jnp.float32).at[slot_token.reshape(-1)].add(expert_grad.reshape(-1, D).astype(jnp.float32))[:SEQUENCE_TOKENS]
    resid_grad = (cotangent.astype(jnp.float32) + routed).astype(jnp.bfloat16)
    decays = jnp.exp(log_decay)
    states = decays * state_before + step_input.astype(jnp.float32)
    gelu_val, gelu_back = jax.vjp(jax.nn.gelu, gate_pre.astype(jnp.float32))
    mixed = (gelu_val * states).astype(jnp.bfloat16)
    d_mixed = jnp.dot(resid_grad, out_proj, preferred_element_type=jnp.float32)
    grad_gate_pre = gelu_back(d_mixed * states)[0].astype(jnp.bfloat16)
    grad_proj = jnp.dot(resid_grad.T, mixed, preferred_element_type=jnp.float32)
    direct = d_mixed * gelu_val
    following = jnp.concatenate([decays[1:], jnp.zeros((1, STATE_CHANNELS), jnp.float32)], axis=0)
    scanned = lax.associative_scan(reverse_link, (jnp.flip(following, 0), jnp.flip(direct, 0)), axis=0)
    grad_step_input = jnp.flip(scanned[1], 0)
    grad_log_decay = grad_step_input * decays * state_before
    return (grad_gate, grad_up, grad_down, grad_proj, grad_gate_pre, grad_step_input, grad_log_decay)
```

```python
import functools
import math

import jax
import jax.numpy as jnp
from jax import lax
from jax.experimental import pallas as pl
from jax.experimental.pallas import tpu as pltpu
from jax.sharding import PartitionSpec as P

F32, BF16 = jnp.float32, jnp.bfloat16
VMEM = pltpu.VMEM
ROOT = math.sqrt(2.0 / math.pi)


def contract(a, b, da, db):
    return lax.dot_general(a, b, (((da,), (db,)), ((), ())), preferred_element_type=F32)


def front_kernel(experts, cap, tp_ref, routes_ref, weight_ref, resid_ref, cot_ref, send_ref, pick_ref, cot_t_ref):
    rows = routes_ref.shape[1]
    width = resid_ref.shape[1]
    r0, r1 = routes_ref[0:1, :], routes_ref[1:2, :]
    w0, w1 = weight_ref[0:1, :], weight_ref[1:2, :]
    ids = lax.broadcasted_iota(jnp.int32, (experts, rows), 0)
    is0, is1 = ids == r0, ids == r1
    named = (jnp.where(is0, 1.0, 0.0) + jnp.where(is1, 1.0, 0.0)).astype(BF16)
    before = lax.broadcasted_iota(jnp.int32, (rows, rows), 0) < lax.broadcasted_iota(jnp.int32, (rows, rows), 1)
    counts = contract(named, jnp.where(before, 1.0, 0.0).astype(BF16), 1, 0)
    slot0 = r0 * cap + jnp.sum(jnp.where(is0, counts, 0.0), axis=0, keepdims=True).astype(jnp.int32)
    slot1 = r1 * cap + jnp.sum(jnp.where(is1, counts, 0.0), axis=0, keepdims=True).astype(jnp.int32)
    resid, cot = resid_ref[...], cot_ref[...]
    part = 8
    for k in range(experts // part):
        size = part * cap
        at = lax.broadcasted_iota(jnp.int32, (size, rows), 0) + k * size
        p0, p1 = at == slot0, at == slot1
        pick = (jnp.where(p0, 1.0, 0.0) + jnp.where(p1, 1.0, 0.0)).astype(BF16)
        pick_ref[k * size : (k + 1) * size, :] = pick
        scale = jnp.sum(jnp.where(p0, w0, 0.0) + jnp.where(p1, w1, 0.0), axis=1, keepdims=True)
        got = contract(pick, resid, 1, 0).astype(BF16)
        cots = (scale * contract(pick, cot, 1, 0)).astype(BF16)
        send_ref[k * part : (k + 1) * part, 0:cap, :] = got.reshape(part, cap, width)
        send_ref[k * part : (k + 1) * part, cap : 2 * cap, :] = cots.reshape(part, cap, width)
    cot_t_ref[...] = cot.astype(F32).T.astype(BF16)


def front(routes_t, weight_t, resid, cotangent, experts, cap, n_tp):
    rows, model = resid.shape
    width = model // n_tp
    tp = lax.axis_index("tp").astype(jnp.int32).reshape(1)
    whole = lambda shape: pl.BlockSpec(shape, lambda i, t: (0,) * len(shape))
    cols = pl.BlockSpec((rows, width), lambda i, t: (0, t[0]))
    return pl.pallas_call(
        functools.partial(front_kernel, experts, cap),
        grid_spec=pltpu.PrefetchScalarGridSpec(
            num_scalar_prefetch=1,
            grid=(1,),
            in_specs=[whole((2, rows)), whole((2, rows)), cols, cols],
            out_specs=[whole((experts, 2 * cap, width)), whole((experts * cap, rows)), whole((width, rows))],
        ),
        out_shape=[
            jax.ShapeDtypeStruct((experts, 2 * cap, width), BF16),
            jax.ShapeDtypeStruct((experts * cap, rows), BF16),
            jax.ShapeDtypeStruct((width, rows), BF16),
        ],
        name="front",
    )(tp, routes_t, weight_t, resid, cotangent)


def shifted(x, by):
    return pltpu.roll(x, x.shape[1] - by, 1)


def reverse_scan(factor, value):
    rows = factor.shape[1]
    lane = lax.broadcasted_iota(jnp.int32, factor.shape, 1)
    by = 1
    while by < rows:
        inside = lane < rows - by
        value = value + factor * jnp.where(inside, shifted(value, by), 0.0)
        factor = factor * jnp.where(inside, shifted(factor, by), 1.0)
        by *= 2
    return factor, value


MESH = pl.DeviceIdType.MESH


def place():
    sp, tp = lax.axis_index("sp"), lax.axis_index("tp")
    z, x, core = lax.div(sp, 4), lax.rem(sp, 4), lax.rem(tp, 2)
    right, left, across = lax.rem(tp + 2, 8), lax.rem(tp + 6, 8), lax.rem(tp + 4, 8)
    return sp, tp, z, x, right, left, across, 1 - 2 * core


def remote(src, dst, send, recv, sp, tp):
    return pltpu.make_async_remote_copy(
        src_ref=src, dst_ref=dst, send_sem=send, recv_sem=recv, device_id={"sp": sp, "tp": tp}, device_id_type=MESH
    )


def greet(peers):
    barrier = pltpu.get_barrier_semaphore()
    for sp, tp in peers:
        pl.semaphore_signal(barrier, inc=1, device_id={"sp": sp, "tp": tp}, device_id_type=MESH)
    return lambda: pl.semaphore_wait(barrier, len(peers))


def tail_kernel(back_ref, pick_ref, cot_t_ref, proj_ref, gate_ref, decay_ref, before_ref, step_ref,
                d_gate_ref, g_step_ref, g_log_ref, g_proj_ref,
                rg, term, from_x, sums, from_z, ends, ends_x, row, ends_z, states, gelu, slope, mixed, dm, prod,
                ag_send, ag_l, ag_r, ag_a, ag_d, x_send, x_recv, z_send, z_recv, e_send, ex_recv, ez_recv):
    sp, tp, z, x, right, left, across, flip = place()
    mate = tp + flip
    channels, rows = gate_ref.shape
    depth = rg.shape[1]
    half_rows = depth // 2
    part = channels // 2
    xs = [z * 4 + lax.rem(x + d, 4) for d in range(1, 4)]
    zs = [lax.rem(z + d, 8) * 4 + x for d in range(1, 8)]
    arrive = greet([(sp, right), (sp, left), (sp, mate)] + [(q, tp) for q in xs + zs])

    slots = pick_ref.shape[0]
    routed = contract(back_ref[...].reshape(slots, depth), pick_ref[...], 0, 0)
    rg[tp] = (cot_t_ref[...].astype(F32) + routed).astype(BF16)
    arrive()

    def half(j, h):
        return rg.at[j, pl.ds(h * half_rows, half_rows), :]

    def moved(ref, k, recv, to):
        return remote(ref, ref, ag_send.at[k], recv, sp, to)

    sent = [
        moved(half(tp, 0), 0, ag_l.at[0], right),
        moved(half(tp, 1), 1, ag_r.at[1], left),
        moved(half(tp, 1), 2, ag_l.at[1], right),
        moved(half(tp, 0), 3, ag_r.at[0], left),
        moved(rg.at[tp], 4, ag_d.at[0], mate),
    ]
    for copy in sent:
        copy.start()

    def prepare(k):
        at = pl.ds(k * part, part)
        v = gate_ref[at, :].astype(F32)
        decays = jnp.exp(decay_ref[at, :])
        state = decays * before_ref[at, :] + step_ref[at, :].astype(F32)
        th = jnp.tanh(ROOT * (v + 0.044715 * (v * v * v)))
        act = 0.5 * v * (1.0 + th)
        gelu[at, :] = act
        states[at, :] = state
        slope[at, :] = 0.5 * (1.0 + th) + 0.5 * v * (1.0 - th * th) * (ROOT * (1.0 + 3.0 * 0.044715 * (v * v)))
        mixed[at, :] = (act * state).astype(BF16)

    def pass_on(ref, k, arrived, recv, to):
        moved(ref, k, arrived, to).wait_recv()
        copy = moved(ref, k, recv, to)
        copy.start()
        sent.append(copy)

    prepare(0)
    pass_on(half(left, 0), 5, ag_l.at[0], ag_a.at[0], right)
    pass_on(half(right, 1), 6, ag_r.at[1], ag_a.at[1], left)
    prepare(1)

    crossing = []

    def use(t, j):
        cols = pl.ds(pl.multiple_of(j * depth, depth), depth)
        piece = rg[j]
        term[j] = contract(piece, mixed[...], 1, 1).astype(BF16).reshape(term.shape[1:])
        for d in range(1, 4):
            to = lax.rem(x + d, 4)
            copy = remote(term.at[j, to], from_x.at[d - 1, j], x_send.at[t, d - 1], x_recv.at[t, d - 1], z * 4 + to, tp)
            copy.start()
            crossing.append(copy)
        product = contract(proj_ref[:, cols], piece, 1, 0)
        dm[...] = product if t == 0 else dm[...] + product

    use(0, tp)
    moved(rg.at[mate], 4, ag_d.at[0], mate).wait_recv()
    use(1, mate)
    moved(half(left, 1), 7, ag_l.at[1], mate).wait_recv()
    copy = moved(rg.at[left], 7, ag_d.at[1], mate)
    copy.start()
    sent.append(copy)
    moved(half(right, 0), 8, ag_r.at[0], mate).wait_recv()
    copy = moved(rg.at[right], 8, ag_d.at[2], mate)
    copy.start()
    sent.append(copy)
    use(2, left)
    use(3, right)
    pass_on(half(across, 0), 9, ag_a.at[0], ag_d.at[3], mate)
    pass_on(half(across, 1), 10, ag_a.at[1], ag_d.at[4], mate)
    moved(rg.at[left + flip], 7, ag_d.at[1], mate).wait_recv()
    use(4, left + flip)
    moved(rg.at[right + flip], 8, ag_d.at[2], mate).wait_recv()
    use(5, right + flip)
    use(6, across)
    moved(half(across + flip, 0), 9, ag_d.at[3], mate).wait_recv()
    moved(half(across + flip, 1), 10, ag_d.at[4], mate).wait_recv()
    use(7, across + flip)
    order = [tp, mate, left, right, left + flip, right + flip, across, across + flip]

    lines = [jnp.zeros((1, channels), F32), jnp.zeros((1, channels), F32)]
    for k in range(2):
        at = pl.ds(k * part, part)
        decays = jnp.exp(decay_ref[at, :])
        d_mixed = dm[at, :]
        d_gate_ref[at, :] = (d_mixed * states[at, :] * slope[at, :]).astype(BF16)
        lane = lax.broadcasted_iota(jnp.int32, decays.shape, 1)
        following = jnp.where(lane < rows - 1, shifted(decays, 1), 1.0)
        products, local = reverse_scan(following, d_mixed * gelu[at, :])
        prod[at, :] = products
        g_step_ref[at, :] = local
        same = lax.broadcasted_iota(jnp.int32, (part, channels), 0) + k * part == lax.broadcasted_iota(
            jnp.int32, (part, channels), 1
        )
        first = decays[:, 0:1]
        for i, ended in enumerate((products, local)):
            lines[i] = lines[i] + jnp.sum(jnp.where(same, first * ended[:, 0:1], 0.0), axis=0, keepdims=True)
    ends[...] = jnp.zeros_like(ends)
    row[...] = jnp.zeros_like(row)
    ends[0:1, :] = lines[0]
    ends[1:2, :] = lines[1]
    ends_x[x] = ends[...]
    passed = []
    for d in range(1, 4):
        copy = remote(ends, ends_x.at[x], e_send.at[d - 1], ex_recv.at[d - 1], z * 4 + lax.rem(x + d, 4), tp)
        copy.start()
        passed.append(copy)

    def cross_sum(t):
        j = order[t]
        total = term[j, x].astype(F32)
        for d in range(1, 4):
            remote(from_x.at[d - 1, j], from_x.at[d - 1, j], x_send.at[t, d - 1], x_recv.at[t, d - 1], sp, mate).wait_recv()
            total = total + from_x[d - 1, j].astype(F32)
        sums[j] = total.astype(BF16)

        @pl.when(j == z)
        def _():
            g_proj_ref[...] = total

        @pl.when(j != z)
        def _():
            remote(sums.at[j], from_z.at[z], z_send.at[j], z_recv.at[z], j * 4 + x, tp).start()

    for t in range(4):
        cross_sum(t)
    scale, shift = jnp.ones((1, channels), F32), jnp.zeros((1, channels), F32)
    for d in range(1, 4):
        q = lax.rem(x + 4 - d, 4)
        remote(ends, ends_x.at[q], e_send.at[d - 1], ex_recv.at[d - 1], sp, mate).wait_recv()
    for q in reversed(range(4)):
        shift = ends_x[q, 1:2, :] + ends_x[q, 0:1, :] * shift
        scale = ends_x[q, 0:1, :] * scale
    row[0:1, :] = scale
    row[1:2, :] = shift
    for d in range(1, 8):
        copy = remote(row, ends_z.at[z], e_send.at[d + 2], ez_recv.at[d - 1], lax.rem(z + d, 8) * 4 + x, tp)
        copy.start()
        passed.append(copy)
    for t in range(4, 8):
        cross_sum(t)
    for d in range(1, 8):
        q = lax.rem(z + 8 - d, 8)
        remote(row, ends_z.at[q], e_send.at[d + 2], ez_recv.at[d - 1], sp, mate).wait_recv()
    ends_z[z] = row[...]
    entering = jnp.zeros((1, channels), F32)
    for q in reversed(range(1, 8)):
        entering = jnp.where(q > z, ends_z[q, 1:2, :] + ends_z[q, 0:1, :] * entering, entering)
    for q in reversed(range(1, 4)):
        entering = jnp.where(q > x, ends_x[q, 1:2, :] + ends_x[q, 0:1, :] * entering, entering)
    for k in range(2):
        at = pl.ds(k * part, part)
        same = lax.broadcasted_iota(jnp.int32, (part, channels), 0) + k * part == lax.broadcasted_iota(
            jnp.int32, (part, channels), 1
        )
        column = jnp.sum(jnp.where(same, entering, 0.0), axis=1, keepdims=True)
        grad = g_step_ref[at, :] + prod[at, :] * column
        g_step_ref[at, :] = grad
        g_log_ref[at, :] = grad * jnp.exp(decay_ref[at, :]) * before_ref[at, :]
    for d in range(1, 8):
        q = lax.rem(z + d, 8)
        remote(from_z.at[q], from_z.at[q], z_send.at[q], z_recv.at[q], sp, mate).wait_recv()
        g_proj_ref[...] += from_z[q].astype(F32)
    for d in range(1, 8):
        q = lax.rem(z + d, 8)
        remote(sums.at[q], from_z.at[z], z_send.at[q], z_recv.at[z], sp, mate).wait_send()
    for copy in sent + crossing + passed:
        copy.wait_send()


def tail(back, pick, cot_t, proj, gate, decay, before, step):
    channels, rows = gate.shape
    depth = cot_t.shape[0]
    flat = (channels, rows)
    lines = 8 * depth // 32
    outs = [(flat, BF16), (flat, F32), (flat, F32), ((lines, channels), F32)]
    dma = pltpu.SemaphoreType.DMA
    return pl.pallas_call(
        tail_kernel,
        in_specs=[pl.BlockSpec(memory_space=VMEM)] * 8,
        out_specs=[pl.BlockSpec(memory_space=VMEM)] * 4,
        out_shape=[jax.ShapeDtypeStruct(s, d) for s, d in outs],
        scratch_shapes=[
            VMEM((8, depth, rows), BF16),
            VMEM((8, 4, lines, channels), BF16),
            VMEM((3, 8, lines, channels), BF16),
            VMEM((8, lines, channels), BF16),
            VMEM((8, lines, channels), BF16),
            VMEM((8, channels), F32),
            VMEM((4, 8, channels), F32),
            VMEM((8, channels), F32),
            VMEM((8, 8, channels), F32),
            VMEM(flat, F32),
            VMEM(flat, F32),
            VMEM(flat, F32),
            VMEM(flat, BF16),
            VMEM(flat, F32),
            VMEM(flat, F32),
            dma((11,)), dma((2,)), dma((2,)), dma((2,)), dma((5,)),
            dma((8, 3)), dma((8, 3)), dma((8,)), dma((8,)), dma((10,)), dma((3,)), dma((7,)),
        ],
        compiler_params=pltpu.CompilerParams(collective_id=1, has_side_effects=True, vmem_limit_bytes=48 << 20),
        name="tail",
    )(back, pick, cot_t, proj, gate, decay, before, step)


def expert_work(in_rows, cot_rows, gate_w, up_w, down_w):
    gate_act = jnp.dot(in_rows, gate_w, preferred_element_type=F32)
    up_act = jnp.dot(in_rows, up_w, preferred_element_type=F32)
    sig = jax.nn.sigmoid(gate_act)
    silu = gate_act * sig
    hidden = (silu * up_act).astype(BF16)
    grad_down = contract(hidden, cot_rows, 0, 0)
    d_hidden = contract(cot_rows, down_w, 1, 1)
    d_gate = (d_hidden * up_act * (sig * (1.0 + gate_act * (1.0 - sig)))).astype(BF16)
    d_up = (d_hidden * silu).astype(BF16)
    grad_gate = contract(in_rows, d_gate, 0, 0)
    grad_up = contract(in_rows, d_up, 0, 0)
    partial_value = contract(d_gate, gate_w, 1, 1) + contract(d_up, up_w, 1, 1)
    return grad_gate[None], grad_up[None], grad_down[None], partial_value.astype(BF16)


def on_device(resid, cotangent, routes, route_weight, w_gate, w_up, w_down, out_proj, gate_pre, log_decay,
              state_before, step_input):
    rows, model = resid.shape
    experts, n_tp = lax.axis_size("sp"), lax.axis_size("tp")
    cap = 2 * rows * routes.shape[1] // experts
    send, pick, cot_t = front(routes.T, route_weight.T, resid, cotangent, experts, cap, n_tp)
    got = lax.all_to_all(send, "sp", split_axis=0, concat_axis=0, tiled=True)
    full = lax.all_gather(got, "tp", axis=2, tiled=True)
    grad_gate, grad_up, grad_down, partial_value = expert_work(
        full[:, :cap].reshape(-1, model), full[:, cap:].reshape(-1, model), w_gate[0], w_up[0], w_down[0]
    )
    summed = lax.psum_scatter(partial_value.reshape(experts, cap, model), "tp", scatter_dimension=2, tiled=True)
    back = lax.all_to_all(summed, "sp", split_axis=0, concat_axis=0, tiled=True)
    d_gate, grad_step, grad_log, grad_proj = tail(
        back, pick, cot_t, out_proj.T, gate_pre.T, log_decay.T, state_before.T, step_input.T
    )
    return grad_gate, grad_up, grad_down, grad_proj, d_gate.T, grad_step.T, grad_log.T


def solution(mesh):
    by_sp, both = P("sp", None), P("sp", "tp")
    cols = P("sp", None, "tp")
    return jax.shard_map(
        on_device,
        mesh=mesh,
        in_specs=(by_sp, by_sp, by_sp, by_sp, cols, cols, P("sp", "tp", None), P(None, "tp"), both, both, both, both),
        out_specs=(cols, cols, P("sp", "tp", None), both, both, both, both),
        check_vma=False,
    )
```

```python
import functools
import math

import jax
import jax.numpy as jnp
from jax import lax
from jax.experimental import pallas as pl
from jax.experimental.pallas import tpu as pltpu
from jax.sharding import PartitionSpec as P

F32, BF16 = jnp.float32, jnp.bfloat16
VMEM = pltpu.VMEM
ROOT = math.sqrt(2.0 / math.pi)


def contract(a, b, da, db):
    return lax.dot_general(a, b, (((da,), (db,)), ((), ())), preferred_element_type=F32)


def front_kernel(experts, cap, tp_ref, routes_ref, weight_ref, resid_ref, cot_ref, send_ref, pick_ref, cot_t_ref):
    rows = routes_ref.shape[1]
    width = resid_ref.shape[1]
    r0, r1 = routes_ref[0:1, :], routes_ref[1:2, :]
    w0, w1 = weight_ref[0:1, :], weight_ref[1:2, :]
    ids = lax.broadcasted_iota(jnp.int32, (experts, rows), 0)
    is0, is1 = ids == r0, ids == r1
    named = (jnp.where(is0, 1.0, 0.0) + jnp.where(is1, 1.0, 0.0)).astype(BF16)
    before = lax.broadcasted_iota(jnp.int32, (rows, rows), 0) < lax.broadcasted_iota(jnp.int32, (rows, rows), 1)
    counts = contract(named, jnp.where(before, 1.0, 0.0).astype(BF16), 1, 0)
    slot0 = r0 * cap + jnp.sum(jnp.where(is0, counts, 0.0), axis=0, keepdims=True).astype(jnp.int32)
    slot1 = r1 * cap + jnp.sum(jnp.where(is1, counts, 0.0), axis=0, keepdims=True).astype(jnp.int32)
    resid, cot = resid_ref[...], cot_ref[...]
    part = 8
    for k in range(experts // part):
        size = part * cap
        at = lax.broadcasted_iota(jnp.int32, (size, rows), 0) + k * size
        p0, p1 = at == slot0, at == slot1
        pick = (jnp.where(p0, 1.0, 0.0) + jnp.where(p1, 1.0, 0.0)).astype(BF16)
        pick_ref[k * size : (k + 1) * size, :] = pick
        scale = jnp.sum(jnp.where(p0, w0, 0.0) + jnp.where(p1, w1, 0.0), axis=1, keepdims=True)
        got = contract(pick, resid, 1, 0).astype(BF16)
        cots = (scale * contract(pick, cot, 1, 0)).astype(BF16)
        send_ref[k * part : (k + 1) * part, 0:cap, :] = got.reshape(part, cap, width)
        send_ref[k * part : (k + 1) * part, cap : 2 * cap, :] = cots.reshape(part, cap, width)
    cot_t_ref[...] = cot.astype(F32).T.astype(BF16)


def front(routes_t, weight_t, resid, cotangent, experts, cap, n_tp):
    rows, model = resid.shape
    width = model // n_tp
    tp = lax.axis_index("tp").astype(jnp.int32).reshape(1)
    whole = lambda shape: pl.BlockSpec(shape, lambda i, t: (0,) * len(shape))
    cols = pl.BlockSpec((rows, width), lambda i, t: (0, t[0]))
    return pl.pallas_call(
        functools.partial(front_kernel, experts, cap),
        grid_spec=pltpu.PrefetchScalarGridSpec(
            num_scalar_prefetch=1,
            grid=(1,),
            in_specs=[whole((2, rows)), whole((2, rows)), cols, cols],
            out_specs=[whole((experts, 2 * cap, width)), whole((experts * cap, rows)), whole((width, rows))],
        ),
        out_shape=[
            jax.ShapeDtypeStruct((experts, 2 * cap, width), BF16),
            jax.ShapeDtypeStruct((experts * cap, rows), BF16),
            jax.ShapeDtypeStruct((width, rows), BF16),
        ],
        name="front",
    )(tp, routes_t, weight_t, resid, cotangent)


def shifted(x, by):
    return pltpu.roll(x, x.shape[1] - by, 1)


def reverse_scan(factor, value):
    rows = factor.shape[1]
    lane = lax.broadcasted_iota(jnp.int32, factor.shape, 1)
    by = 1
    while by < rows:
        inside = lane < rows - by
        value = value + factor * jnp.where(inside, shifted(value, by), 0.0)
        factor = factor * jnp.where(inside, shifted(factor, by), 1.0)
        by *= 2
    return factor, value


MESH = pl.DeviceIdType.MESH


def place():
    sp, tp = lax.axis_index("sp"), lax.axis_index("tp")
    z, x, core = lax.div(sp, 4), lax.rem(sp, 4), lax.rem(tp, 2)
    right, left, across = lax.rem(tp + 2, 8), lax.rem(tp + 6, 8), lax.rem(tp + 4, 8)
    return sp, tp, z, x, right, left, across, 1 - 2 * core


def remote(src, dst, send, recv, sp, tp):
    return pltpu.make_async_remote_copy(
        src_ref=src, dst_ref=dst, send_sem=send, recv_sem=recv, device_id={"sp": sp, "tp": tp}, device_id_type=MESH
    )


def greet(peers):
    barrier = pltpu.get_barrier_semaphore()
    for sp, tp in peers:
        pl.semaphore_signal(barrier, inc=1, device_id={"sp": sp, "tp": tp}, device_id_type=MESH)
    return lambda: pl.semaphore_wait(barrier, len(peers))


def tail_kernel(back_ref, pick_ref, cot_t_ref, proj_ref, gate_ref, decay_ref, before_ref, step_ref,
                d_gate_ref, g_step_ref, g_log_ref, g_proj_ref,
                rg, term, from_x, sums, from_z, ends, ends_x, row, ends_z, states, gelu, slope, mixed, dm, prod,
                ag_send, ag_l, ag_r, ag_a, ag_d, x_send, x_recv, z_send, z_recv, e_send, ex_recv, ez_recv):
    sp, tp, z, x, right, left, across, flip = place()
    mate = tp + flip
    channels, rows = gate_ref.shape
    depth = rg.shape[1]
    half_rows = depth // 2
    part = channels // 2
    xs = [z * 4 + lax.rem(x + d, 4) for d in range(1, 4)]
    zs = [lax.rem(z + d, 8) * 4 + x for d in range(1, 8)]
    arrive = greet([(sp, right), (sp, left), (sp, mate)] + [(q, tp) for q in xs + zs])

    slots = pick_ref.shape[0]
    routed = contract(back_ref[...].reshape(slots, depth), pick_ref[...], 0, 0)
    rg[tp] = (cot_t_ref[...].astype(F32) + routed).astype(BF16)
    arrive()

    def half(j, h):
        return rg.at[j, pl.ds(h * half_rows, half_rows), :]

    def moved(ref, k, recv, to):
        return remote(ref, ref, ag_send.at[k], recv, sp, to)

    sent = [
        moved(half(tp, 0), 0, ag_l.at[0], right),
        moved(half(tp, 1), 1, ag_r.at[1], left),
        moved(half(tp, 1), 2, ag_l.at[1], right),
        moved(half(tp, 0), 3, ag_r.at[0], left),
        moved(rg.at[tp], 4, ag_d.at[0], mate),
    ]
    for copy in sent:
        copy.start()

    def prepare(k):
        at = pl.ds(k * part, part)
        v = gate_ref[at, :].astype(F32)
        decays = jnp.exp(decay_ref[at, :])
        state = decays * before_ref[at, :] + step_ref[at, :].astype(F32)
        th = jnp.tanh(ROOT * (v + 0.044715 * (v * v * v)))
        act = 0.5 * v * (1.0 + th)
        gelu[at, :] = act
        states[at, :] = state
        slope[at, :] = 0.5 * (1.0 + th) + 0.5 * v * (1.0 - th * th) * (ROOT * (1.0 + 3.0 * 0.044715 * (v * v)))
        mixed[at, :] = (act * state).astype(BF16)

    def pass_on(ref, k, arrived, recv, to):
        moved(ref, k, arrived, to).wait_recv()
        copy = moved(ref, k, recv, to)
        copy.start()
        sent.append(copy)

    prepare(0)
    pass_on(half(left, 0), 5, ag_l.at[0], ag_a.at[0], right)
    pass_on(half(right, 1), 6, ag_r.at[1], ag_a.at[1], left)
    prepare(1)

    crossing = []

    def use(t, j):
        cols = pl.ds(pl.multiple_of(j * depth, depth), depth)
        piece = rg[j]
        term[j] = contract(piece, mixed[...], 1, 1).astype(BF16).reshape(term.shape[1:])
        for d in range(1, 4):
            to = lax.rem(x + d, 4)
            copy = remote(term.at[j, to], from_x.at[d - 1, j], x_send.at[t, d - 1], x_recv.at[t, d - 1], z * 4 + to, tp)
            copy.start()
            crossing.append(copy)
        product = contract(proj_ref[:, cols], piece, 1, 0)
        dm[...] = product if t == 0 else dm[...] + product

    use(0, tp)
    moved(rg.at[mate], 4, ag_d.at[0], mate).wait_recv()
    use(1, mate)
    moved(half(left, 1), 7, ag_l.at[1], mate).wait_recv()
    copy = moved(rg.at[left], 7, ag_d.at[1], mate)
    copy.start()
    sent.append(copy)
    moved(half(right, 0), 8, ag_r.at[0], mate).wait_recv()
    copy = moved(rg.at[right], 8, ag_d.at[2], mate)
    copy.start()
    sent.append(copy)
    use(2, left)
    use(3, right)
    pass_on(half(across, 0), 9, ag_a.at[0], ag_d.at[3], mate)
    pass_on(half(across, 1), 10, ag_a.at[1], ag_d.at[4], mate)
    moved(rg.at[left + flip], 7, ag_d.at[1], mate).wait_recv()
    use(4, left + flip)
    moved(rg.at[right + flip], 8, ag_d.at[2], mate).wait_recv()
    use(5, right + flip)
    use(6, across)
    moved(half(across + flip, 0), 9, ag_d.at[3], mate).wait_recv()
    moved(half(across + flip, 1), 10, ag_d.at[4], mate).wait_recv()
    use(7, across + flip)
    order = [tp, mate, left, right, left + flip, right + flip, across, across + flip]

    lines = [jnp.zeros((1, channels), F32), jnp.zeros((1, channels), F32)]
    for k in range(2):
        at = pl.ds(k * part, part)
        decays = jnp.exp(decay_ref[at, :])
        d_mixed = dm[at, :]
        d_gate_ref[at, :] = (d_mixed * states[at, :] * slope[at, :]).astype(BF16)
        lane = lax.broadcasted_iota(jnp.int32, decays.shape, 1)
        following = jnp.where(lane < rows - 1, shifted(decays, 1), 1.0)
        products, local = reverse_scan(following, d_mixed * gelu[at, :])
        prod[at, :] = products
        g_step_ref[at, :] = local
        same = lax.broadcasted_iota(jnp.int32, (part, channels), 0) + k * part == lax.broadcasted_iota(
            jnp.int32, (part, channels), 1
        )
        first = decays[:, 0:1]
        for i, ended in enumerate((products, local)):
            lines[i] = lines[i] + jnp.sum(jnp.where(same, first * ended[:, 0:1], 0.0), axis=0, keepdims=True)
    ends[...] = jnp.zeros_like(ends)
    row[...] = jnp.zeros_like(row)
    ends[0:1, :] = lines[0]
    ends[1:2, :] = lines[1]
    ends_x[x] = ends[...]
    passed = []
    for d in range(1, 4):
        copy = remote(ends, ends_x.at[x], e_send.at[d - 1], ex_recv.at[d - 1], z * 4 + lax.rem(x + d, 4), tp)
        copy.start()
        passed.append(copy)

    def cross_sum(t):
        j = order[t]
        total = term[j, x].astype(F32)
        for d in range(1, 4):
            remote(from_x.at[d - 1, j], from_x.at[d - 1, j], x_send.at[t, d - 1], x_recv.at[t, d - 1], sp, mate).wait_recv()
            total = total + from_x[d - 1, j].astype(F32)
        sums[j] = total.astype(BF16)

        @pl.when(j == z)
        def _():
            g_proj_ref[...] = total

        @pl.when(j != z)
        def _():
            remote(sums.at[j], from_z.at[z], z_send.at[j], z_recv.at[z], j * 4 + x, tp).start()

    for t in range(4):
        cross_sum(t)
    scale, shift = jnp.ones((1, channels), F32), jnp.zeros((1, channels), F32)
    for d in range(1, 4):
        q = lax.rem(x + 4 - d, 4)
        remote(ends, ends_x.at[q], e_send.at[d - 1], ex_recv.at[d - 1], sp, mate).wait_recv()
    for q in reversed(range(4)):
        shift = ends_x[q, 1:2, :] + ends_x[q, 0:1, :] * shift
        scale = ends_x[q, 0:1, :] * scale
    row[0:1, :] = scale
    row[1:2, :] = shift
    for d in range(1, 8):
        copy = remote(row, ends_z.at[z], e_send.at[d + 2], ez_recv.at[d - 1], lax.rem(z + d, 8) * 4 + x, tp)
        copy.start()
        passed.append(copy)
    for t in range(4, 8):
        cross_sum(t)
    for d in range(1, 8):
        q = lax.rem(z + 8 - d, 8)
        remote(row, ends_z.at[q], e_send.at[d + 2], ez_recv.at[d - 1], sp, mate).wait_recv()
    ends_z[z] = row[...]
    entering = jnp.zeros((1, channels), F32)
    for q in reversed(range(1, 8)):
        entering = jnp.where(q > z, ends_z[q, 1:2, :] + ends_z[q, 0:1, :] * entering, entering)
    for q in reversed(range(1, 4)):
        entering = jnp.where(q > x, ends_x[q, 1:2, :] + ends_x[q, 0:1, :] * entering, entering)
    for k in range(2):
        at = pl.ds(k * part, part)
        same = lax.broadcasted_iota(jnp.int32, (part, channels), 0) + k * part == lax.broadcasted_iota(
            jnp.int32, (part, channels), 1
        )
        column = jnp.sum(jnp.where(same, entering, 0.0), axis=1, keepdims=True)
        grad = g_step_ref[at, :] + prod[at, :] * column
        g_step_ref[at, :] = grad
        g_log_ref[at, :] = grad * jnp.exp(decay_ref[at, :]) * before_ref[at, :]
    for d in range(1, 8):
        q = lax.rem(z + d, 8)
        remote(from_z.at[q], from_z.at[q], z_send.at[q], z_recv.at[q], sp, mate).wait_recv()
        g_proj_ref[...] += from_z[q].astype(F32)
    for d in range(1, 8):
        q = lax.rem(z + d, 8)
        remote(sums.at[q], from_z.at[z], z_send.at[q], z_recv.at[z], sp, mate).wait_send()
    for copy in sent + crossing + passed:
        copy.wait_send()


def tail(back, pick, cot_t, proj, gate, decay, before, step):
    channels, rows = gate.shape
    depth = cot_t.shape[0]
    flat = (channels, rows)
    lines = 8 * depth // 32
    outs = [(flat, BF16), (flat, F32), (flat, F32), ((lines, channels), F32)]
    dma = pltpu.SemaphoreType.DMA
    return pl.pallas_call(
        tail_kernel,
        in_specs=[pl.BlockSpec(memory_space=VMEM)] * 8,
        out_specs=[pl.BlockSpec(memory_space=VMEM)] * 4,
        out_shape=[jax.ShapeDtypeStruct(s, d) for s, d in outs],
        scratch_shapes=[
            VMEM((8, depth, rows), BF16),
            VMEM((8, 4, lines, channels), BF16),
            VMEM((3, 8, lines, channels), BF16),
            VMEM((8, lines, channels), BF16),
            VMEM((8, lines, channels), BF16),
            VMEM((8, channels), F32),
            VMEM((4, 8, channels), F32),
            VMEM((8, channels), F32),
            VMEM((8, 8, channels), F32),
            VMEM(flat, F32),
            VMEM(flat, F32),
            VMEM(flat, F32),
            VMEM(flat, BF16),
            VMEM(flat, F32),
            VMEM(flat, F32),
            dma((11,)), dma((2,)), dma((2,)), dma((2,)), dma((5,)),
            dma((8, 3)), dma((8, 3)), dma((8,)), dma((8,)), dma((10,)), dma((3,)), dma((7,)),
        ],
        compiler_params=pltpu.CompilerParams(collective_id=1, has_side_effects=True, vmem_limit_bytes=48 << 20),
        name="tail",
    )(back, pick, cot_t, proj, gate, decay, before, step)


N_SENDS = 13


def experts_kernel(send_ref, w_gate_ref, w_up_ref, w_down_ref,
                   g_gate_ref, g_up_ref, g_down_ref, back_ref,
                   buf, w_cat, w_cat_t, w_down_t, acc_t, parts, from_mate, pair, from_far, from_left, from_right, ret, back,
                   a_send, a_recv, sends, yl, yr, ya, ym, pm, fa, fl, fr, b_send, b_recv):
    sp, tp, z, x, right, left, across, flip = place()
    mate = tp + flip
    core = lax.rem(tp, 2)
    y = lax.div(tp, 2)
    y_right, y_left, y_far = lax.rem(y + 1, 4), lax.rem(y + 3, 4), lax.rem(y + 2, 4)
    n_sp, both_caps, depth = send_ref.shape
    cap = both_caps // 2
    steps = n_sp // 4
    arrive = greet([(lax.rem(sp + k, n_sp), tp) for k in range(1, n_sp)] + [(sp, right), (sp, left), (sp, mate)])

    def dz(s):
        h = lax.div(s + 1, 2)
        return lax.rem(jnp.where(lax.rem(s, 2) == 1, h, steps - h), steps)

    def group(s):
        return lax.rem(z + dz(s), steps)

    def toward(s, d):
        return lax.rem(z - dz(s) + steps, steps) * 4 + lax.rem(x + d, 4)

    def out_copy(s, d):
        to = toward(s, d)
        return remote(send_ref.at[to], buf.at[tp, sp], a_send.at[s, d], a_recv.at[s, d], to, tp)

    def back_copy(s, d):
        to = group(s) * 4 + lax.rem(x + d, 4)
        return remote(ret.at[to], back.at[sp], b_send.at[s, d], b_recv.at[s, d], to, tp)

    arrive()
    pltpu.make_async_copy(send_ref.at[sp], buf.at[tp, sp], a_recv.at[0, 0]).start()
    for d in range(1, 4):
        out_copy(0, d).start()

    @pl.loop(1, steps)
    def _(s):
        for d in range(4):
            out_copy(s, d).start()

    def wait(ref, sem):
        remote(ref, ref, a_send.at[0, 0], sem, sp, mate).wait_recv()

    w_cat[:, 0:128] = w_gate_ref[...]
    w_cat[:, 128:256] = w_up_ref[...]
    acc_t[...] = jnp.zeros_like(acc_t)
    g_down_ref[...] = jnp.zeros_like(g_down_ref)

    @pl.loop(0, 8)
    def _(j):
        at = pl.ds(pl.multiple_of(j * depth, depth), depth)
        w_cat_t[:, at] = w_cat[at, :].astype(F32).T.astype(BF16)
        w_down_t[at, :] = w_down_ref[:, at].astype(F32).T.astype(BF16)

    def four(s):
        return pl.ds(group(s) * 4, 4)

    def two(s, h):
        return pl.ds(group(s) * 4 + 2 * h, 2)

    def sends_of(s, first, last):
        blk = four(s)
        makers = [
            lambda: remote(buf.at[tp, blk], buf.at[tp, blk], sends.at[s, 0], yl.at[s], sp, right),
            lambda: remote(buf.at[tp, blk], buf.at[tp, blk], sends.at[s, 1], yr.at[s], sp, left),
            lambda: remote(buf.at[tp, blk], buf.at[tp, blk], sends.at[s, 2], ym.at[s, 0], sp, mate),
            lambda: remote(buf.at[left, two(s, 0)], buf.at[left, two(s, 0)], sends.at[s, 3], ya.at[s, 0], sp, right),
            lambda: remote(buf.at[right, two(s, 1)], buf.at[right, two(s, 1)], sends.at[s, 4], ya.at[s, 1], sp, left),
            lambda: remote(buf.at[left, blk], buf.at[left, blk], sends.at[s, 5], ym.at[s, 1], sp, mate),
            lambda: remote(buf.at[right, blk], buf.at[right, blk], sends.at[s, 6], ym.at[s, 2], sp, mate),
            lambda: remote(buf.at[across, blk], buf.at[across, blk], sends.at[s, 7], ym.at[s, 3], sp, mate),
            lambda: remote(parts.at[1 - core, :, blk], from_mate.at[:, blk], sends.at[s, 8], pm.at[s], sp, mate),
            lambda: remote(pair.at[y_far, two(s, 0)], from_far.at[two(s, 0)], sends.at[s, 9], fa.at[s, 0], sp, right),
            lambda: remote(pair.at[y_far, two(s, 1)], from_far.at[two(s, 1)], sends.at[s, 10], fa.at[s, 1], sp, left),
            lambda: remote(pair.at[y_right, blk], from_left.at[blk], sends.at[s, 11], fl.at[s], sp, right),
            lambda: remote(pair.at[y_left, blk], from_right.at[blk], sends.at[s, 12], fr.at[s], sp, left),
        ]
        return [make() for make in makers[first:last]]

    def spread(s):
        for d in range(4):
            q = group(s) * 4 + lax.rem(x + 4 - d, 4)
            wait(buf.at[tp, q], a_recv.at[s, d])
        for copy in sends_of(s, 0, 3):
            copy.start()

    def forward(s):
        wait(buf.at[left, four(s)], yl.at[s])
        wait(buf.at[right, four(s)], yr.at[s])
        for copy in sends_of(s, 3, 7):
            copy.start()

    def hand_over(s):
        wait(buf.at[across, two(s, 0)], ya.at[s, 0])
        wait(buf.at[across, two(s, 1)], ya.at[s, 1])
        sends_of(s, 7, 8)[0].start()

    def compute(s):
        blk = four(s)
        for k, j in enumerate((tp, left, right, across)):
            wait(buf.at[j + flip, blk], ym.at[s, k])
        size = 4 * cap

        def rows_of(j):
            return buf[j, blk, 0:cap, :].reshape(size, depth)

        def cots_of(j):
            return buf[j, blk, cap : 2 * cap, :].reshape(size, depth)

        act = jnp.zeros((size, 256), F32)
        d_hidden = jnp.zeros((size, 128), F32)
        for j in range(8):
            cols = slice(j * depth, (j + 1) * depth)
            act = act + contract(rows_of(j), w_cat[cols, :], 1, 0)
            d_hidden = d_hidden + contract(cots_of(j), w_down_t[cols, :], 1, 0)
        gate_act, up_act = act[:, 0:128], act[:, 128:256]
        sig = jax.nn.sigmoid(gate_act)
        silu = gate_act * sig
        hidden = (silu * up_act).astype(BF16)
        d_gate = (d_hidden * up_act * (sig * (1.0 + gate_act * (1.0 - sig)))).astype(BF16)
        d_up = (d_hidden * silu).astype(BF16)
        d_both = jnp.concatenate([d_gate, d_up], axis=1)
        d_both_t = d_both.astype(F32).T.astype(BF16)
        hidden_t = hidden.astype(F32).T.astype(BF16)
        for j in range(8):
            cols = slice(j * depth, (j + 1) * depth)
            value = contract(d_both, w_cat_t[:, cols], 1, 0).astype(BF16)
            parts[j % 2, j // 2, blk] = value.reshape(4, cap, depth)
        sends_of(s, 8, 9)[0].start()
        for j in range(8):
            cols = slice(j * depth, (j + 1) * depth)
            acc_t[:, cols] += contract(d_both_t, rows_of(j), 1, 0)
            g_down_ref[:, cols] += contract(hidden_t, cots_of(j), 1, 0)

    def pair_up(s):
        blk = four(s)
        wait(from_mate.at[:, blk], pm.at[s])
        for k in range(4):
            pair[k, blk] = (parts[core, k, blk].astype(F32) + from_mate[k, blk].astype(F32)).astype(BF16)
        for copy in sends_of(s, 9, 11):
            copy.start()

    def join(s):
        wait(from_far.at[two(s, 0)], fa.at[s, 0])
        wait(from_far.at[two(s, 1)], fa.at[s, 1])
        for k, h in ((y_right, 0), (y_left, 1)):
            at = two(s, h)
            pair[k, at] = (pair[k, at].astype(F32) + from_far[at].astype(F32)).astype(BF16)
        for copy in sends_of(s, 11, 13):
            copy.start()

    def finish(s):
        blk = four(s)
        wait(from_left.at[blk], fl.at[s])
        wait(from_right.at[blk], fr.at[s])
        ret[blk] = (pair[y, blk].astype(F32) + from_left[blk].astype(F32) + from_right[blk].astype(F32)).astype(BF16)

        @pl.when(s == 0)
        def _():
            pltpu.make_async_copy(ret.at[sp], back.at[sp], b_recv.at[0, 0]).start()

        @pl.when(s > 0)
        def _():
            back_copy(s, 0).start()

        for d in range(1, 4):
            back_copy(s, d).start()

    stages = ((spread, 0), (forward, 1), (hand_over, 2), (finish, 6), (join, 5), (pair_up, 4), (compute, 3))

    @pl.loop(0, steps + 6)
    def _(t):
        for stage, late in stages:
            @pl.when((t >= late) & (t < steps + late))
            def _():
                stage(t - late)

    for j in range(8):
        cols = slice(j * depth, (j + 1) * depth)
        both = acc_t[:, cols].T
        g_gate_ref[cols, :] = both[:, 0:128]
        g_up_ref[cols, :] = both[:, 128:256]

    @pl.loop(0, steps)
    def _(s):
        for d in range(4):
            q = lax.rem(z - dz(s) + steps, steps) * 4 + lax.rem(x + 4 - d, 4)
            wait(back.at[q], b_recv.at[s, d])

    back_ref[...] = back[...]

    @pl.loop(0, steps)
    def _(s):
        for copy in sends_of(s, 0, N_SENDS):
            copy.wait_send()
        for d in range(1, 4):
            out_copy(s, d).wait_send()
            back_copy(s, d).wait_send()

        @pl.when(s > 0)
        def _():
            out_copy(s, 0).wait_send()
            back_copy(s, 0).wait_send()


def experts_pass(send, w_gate, w_up, w_down):
    n_sp, both_caps, depth = send.shape
    model, units = w_gate.shape
    cap = both_caps // 2
    block = (n_sp, cap, depth)
    steps = n_sp // 4
    dma = pltpu.SemaphoreType.DMA
    outs = [((model, units), F32), ((model, units), F32), ((units, model), F32), (block, BF16)]
    return pl.pallas_call(
        experts_kernel,
        in_specs=[pl.BlockSpec(memory_space=VMEM)] * 4,
        out_specs=[pl.BlockSpec(memory_space=VMEM)] * 4,
        out_shape=[jax.ShapeDtypeStruct(s, d) for s, d in outs],
        scratch_shapes=[
            VMEM((8, n_sp, both_caps, depth), BF16),
            VMEM((model, 2 * units), BF16),
            VMEM((2 * units, model), BF16),
            VMEM((model, units), BF16),
            VMEM((2 * units, model), F32),
            VMEM((2, 4, *block), BF16),
            VMEM((4, *block), BF16),
            VMEM((4, *block), BF16),
            VMEM(block, BF16),
            VMEM(block, BF16),
            VMEM(block, BF16),
            VMEM(block, BF16),
            VMEM(block, BF16),
            dma((steps, 4)), dma((steps, 4)), dma((steps, N_SENDS)),
            dma((steps,)), dma((steps,)), dma((steps, 2)), dma((steps, 4)), dma((steps,)), dma((steps, 2)),
            dma((steps,)), dma((steps,)), dma((steps, 4)), dma((steps, 4)),
        ],
        compiler_params=pltpu.CompilerParams(collective_id=0, has_side_effects=True, vmem_limit_bytes=60 << 20),
        name="experts",
    )(send, w_gate, w_up, w_down)


def on_device(resid, cotangent, routes, route_weight, w_gate, w_up, w_down, out_proj, gate_pre, log_decay,
              state_before, step_input):
    rows, model = resid.shape
    experts, n_tp = lax.axis_size("sp"), lax.axis_size("tp")
    cap = 2 * rows * routes.shape[1] // experts
    send, pick, cot_t = front(routes.T, route_weight.T, resid, cotangent, experts, cap, n_tp)
    grad_gate, grad_up, grad_down, back = experts_pass(send, w_gate[0], w_up[0], w_down[0])
    d_gate, grad_step, grad_log, grad_proj = tail(
        back, pick, cot_t, out_proj.T, gate_pre.T, log_decay.T, state_before.T, step_input.T
    )
    return grad_gate[None], grad_up[None], grad_down[None], grad_proj, d_gate.T, grad_step.T, grad_log.T


def solution(mesh):
    by_sp, both = P("sp", None), P("sp", "tp")
    cols = P("sp", None, "tp")
    return jax.shard_map(
        on_device,
        mesh=mesh,
        in_specs=(by_sp, by_sp, by_sp, by_sp, cols, cols, P("sp", "tp", None), P(None, "tp"), both, both, both, both),
        out_specs=(cols, cols, P("sp", "tp", None), both, both, both, both),
        check_vma=False,
    )
```

```python
import functools
import math

import jax
import jax.numpy as jnp
from jax import lax
from jax.experimental import pallas as pl
from jax.experimental.pallas import tpu as pltpu
from jax.sharding import PartitionSpec as P

F32, BF16 = jnp.float32, jnp.bfloat16
VMEM = pltpu.VMEM
ROOT = math.sqrt(2.0 / math.pi)


def contract(a, b, da, db):
    return lax.dot_general(a, b, (((da,), (db,)), ((), ())), preferred_element_type=F32)


def front_kernel(experts, cap, tp_ref, routes_ref, weight_ref, resid_ref, cot_ref, resid_far_ref, cot_far_ref,
                 send_ref, pick_ref, cot_t_ref):
    rows = routes_ref.shape[1]
    width = resid_ref.shape[1]
    r0, r1 = routes_ref[0:1, :], routes_ref[1:2, :]
    w0, w1 = weight_ref[0:1, :], weight_ref[1:2, :]
    ids = lax.broadcasted_iota(jnp.int32, (experts, rows), 0)
    is0, is1 = ids == r0, ids == r1
    named = (jnp.where(is0, 1.0, 0.0) + jnp.where(is1, 1.0, 0.0)).astype(BF16)
    before = lax.broadcasted_iota(jnp.int32, (rows, rows), 0) < lax.broadcasted_iota(jnp.int32, (rows, rows), 1)
    counts = contract(named, jnp.where(before, 1.0, 0.0).astype(BF16), 1, 0)
    slot0 = r0 * cap + jnp.sum(jnp.where(is0, counts, 0.0), axis=0, keepdims=True).astype(jnp.int32)
    slot1 = r1 * cap + jnp.sum(jnp.where(is1, counts, 0.0), axis=0, keepdims=True).astype(jnp.int32)
    part = 8
    for k in range(experts // part):
        size = part * cap
        at = lax.broadcasted_iota(jnp.int32, (size, rows), 0) + k * size
        p0, p1 = at == slot0, at == slot1
        pick = (jnp.where(p0, 1.0, 0.0) + jnp.where(p1, 1.0, 0.0)).astype(BF16)
        pick_ref[k * size : (k + 1) * size, :] = pick
        scale = jnp.sum(jnp.where(p0, w0, 0.0) + jnp.where(p1, w1, 0.0), axis=1, keepdims=True)
        at = slice(k * part, (k + 1) * part)
        for i, (resid, cot) in enumerate(((resid_ref, cot_ref), (resid_far_ref, cot_far_ref))):
            got = contract(pick, resid[...], 1, 0).astype(BF16)
            cots = (scale * contract(pick, cot[...], 1, 0)).astype(BF16)
            send_ref[i, at, 0:cap, :] = got.reshape(part, cap, width)
            send_ref[i, at, cap : 2 * cap, :] = cots.reshape(part, cap, width)
    cot_t_ref[...] = cot_ref[...].astype(F32).T.astype(BF16)


def front(routes_t, weight_t, resid, cotangent, experts, cap, n_tp):
    rows, model = resid.shape
    width = model // n_tp
    tp = lax.axis_index("tp").astype(jnp.int32)
    slices = jnp.stack([tp, lax.rem(tp + n_tp // 2, n_tp)])
    whole = lambda shape: pl.BlockSpec(shape, lambda i, t: (0,) * len(shape))
    cols = pl.BlockSpec((rows, width), lambda i, t: (0, t[0]))
    far = pl.BlockSpec((rows, width), lambda i, t: (0, t[1]))
    return pl.pallas_call(
        functools.partial(front_kernel, experts, cap),
        grid_spec=pltpu.PrefetchScalarGridSpec(
            num_scalar_prefetch=1,
            grid=(1,),
            in_specs=[whole((2, rows)), whole((2, rows)), cols, cols, far, far],
            out_specs=[whole((2, experts, 2 * cap, width)), whole((experts * cap, rows)), whole((width, rows))],
        ),
        out_shape=[
            jax.ShapeDtypeStruct((2, experts, 2 * cap, width), BF16),
            jax.ShapeDtypeStruct((experts * cap, rows), BF16),
            jax.ShapeDtypeStruct((width, rows), BF16),
        ],
        name="front",
    )(slices, routes_t, weight_t, resid, cotangent, resid, cotangent)


def shifted(x, by):
    return pltpu.roll(x, x.shape[1] - by, 1)


def reverse_scan(factor, value):
    rows = factor.shape[1]
    lane = lax.broadcasted_iota(jnp.int32, factor.shape, 1)
    by = 1
    while by < rows:
        inside = lane < rows - by
        value = value + factor * jnp.where(inside, shifted(value, by), 0.0)
        factor = factor * jnp.where(inside, shifted(factor, by), 1.0)
        by *= 2
    return factor, value


MESH = pl.DeviceIdType.MESH


def place():
    sp, tp = lax.axis_index("sp"), lax.axis_index("tp")
    z, x, core = lax.div(sp, 4), lax.rem(sp, 4), lax.rem(tp, 2)
    right, left, across = lax.rem(tp + 2, 8), lax.rem(tp + 6, 8), lax.rem(tp + 4, 8)
    return sp, tp, z, x, right, left, across, 1 - 2 * core


def remote(src, dst, send, recv, sp, tp):
    return pltpu.make_async_remote_copy(
        src_ref=src, dst_ref=dst, send_sem=send, recv_sem=recv, device_id={"sp": sp, "tp": tp}, device_id_type=MESH
    )


def greet(peers):
    barrier = pltpu.get_barrier_semaphore()
    for sp, tp in peers:
        pl.semaphore_signal(barrier, inc=1, device_id={"sp": sp, "tp": tp}, device_id_type=MESH)
    return lambda: pl.semaphore_wait(barrier, len(peers))


def tail_kernel(back_ref, pick_ref, cot_t_ref, proj_ref, gate_ref, decay_ref, before_ref, step_ref,
                d_gate_ref, g_step_ref, g_log_ref, g_proj_ref,
                rg, term, from_x, sums, from_z, ends, ends_x, row, ends_z, states, gelu, slope, mixed, dm, prod,
                ag_send, ag_l, ag_r, ag_a, ag_d, x_send, x_recv, z_send, z_recv, e_send, ex_recv, ez_recv):
    sp, tp, z, x, right, left, across, flip = place()
    mate = tp + flip
    channels, rows = gate_ref.shape
    depth = rg.shape[1]
    half_rows = depth // 2
    part = channels // 2
    xs = [z * 4 + lax.rem(x + d, 4) for d in range(1, 4)]
    zs = [lax.rem(z + d, 8) * 4 + x for d in range(1, 8)]
    arrive = greet([(sp, right), (sp, left), (sp, mate)] + [(q, tp) for q in xs + zs])

    slots = pick_ref.shape[0]
    routed = contract(back_ref[...].reshape(slots, depth), pick_ref[...], 0, 0)
    rg[tp] = (cot_t_ref[...].astype(F32) + routed).astype(BF16)
    arrive()

    def half(j, h):
        return rg.at[j, pl.ds(h * half_rows, half_rows), :]

    def moved(ref, k, recv, to):
        return remote(ref, ref, ag_send.at[k], recv, sp, to)

    sent = [
        moved(half(tp, 0), 0, ag_l.at[0], right),
        moved(half(tp, 1), 1, ag_r.at[1], left),
        moved(half(tp, 1), 2, ag_l.at[1], right),
        moved(half(tp, 0), 3, ag_r.at[0], left),
        moved(rg.at[tp], 4, ag_d.at[0], mate),
    ]
    for copy in sent:
        copy.start()

    def prepare(k):
        at = pl.ds(k * part, part)
        v = gate_ref[at, :].astype(F32)
        decays = jnp.exp(decay_ref[at, :])
        state = decays * before_ref[at, :] + step_ref[at, :].astype(F32)
        th = jnp.tanh(ROOT * (v + 0.044715 * (v * v * v)))
        act = 0.5 * v * (1.0 + th)
        gelu[at, :] = act
        states[at, :] = state
        slope[at, :] = 0.5 * (1.0 + th) + 0.5 * v * (1.0 - th * th) * (ROOT * (1.0 + 3.0 * 0.044715 * (v * v)))
        mixed[at, :] = (act * state).astype(BF16)

    def pass_on(ref, k, arrived, recv, to):
        moved(ref, k, arrived, to).wait_recv()
        copy = moved(ref, k, recv, to)
        copy.start()
        sent.append(copy)

    prepare(0)
    pass_on(half(left, 0), 5, ag_l.at[0], ag_a.at[0], right)
    pass_on(half(right, 1), 6, ag_r.at[1], ag_a.at[1], left)
    prepare(1)

    crossing = []

    def use(t, j):
        cols = pl.ds(pl.multiple_of(j * depth, depth), depth)
        piece = rg[j]
        term[j] = contract(piece, mixed[...], 1, 1).astype(BF16).reshape(term.shape[1:])
        for d in range(1, 4):
            to = lax.rem(x + d, 4)
            copy = remote(term.at[j, to], from_x.at[d - 1, j], x_send.at[t, d - 1], x_recv.at[t, d - 1], z * 4 + to, tp)
            copy.start()
            crossing.append(copy)
        product = contract(proj_ref[:, cols], piece, 1, 0)
        dm[...] = product if t == 0 else dm[...] + product

    use(0, tp)
    moved(rg.at[mate], 4, ag_d.at[0], mate).wait_recv()
    use(1, mate)
    moved(half(left, 1), 7, ag_l.at[1], mate).wait_recv()
    copy = moved(rg.at[left], 7, ag_d.at[1], mate)
    copy.start()
    sent.append(copy)
    moved(half(right, 0), 8, ag_r.at[0], mate).wait_recv()
    copy = moved(rg.at[right], 8, ag_d.at[2], mate)
    copy.start()
    sent.append(copy)
    use(2, left)
    use(3, right)
    pass_on(half(across, 0), 9, ag_a.at[0], ag_d.at[3], mate)
    pass_on(half(across, 1), 10, ag_a.at[1], ag_d.at[4], mate)
    moved(rg.at[left + flip], 7, ag_d.at[1], mate).wait_recv()
    use(4, left + flip)
    moved(rg.at[right + flip], 8, ag_d.at[2], mate).wait_recv()
    use(5, right + flip)
    use(6, across)
    moved(half(across + flip, 0), 9, ag_d.at[3], mate).wait_recv()
    moved(half(across + flip, 1), 10, ag_d.at[4], mate).wait_recv()
    use(7, across + flip)
    order = [tp, mate, left, right, left + flip, right + flip, across, across + flip]

    lines = [jnp.zeros((1, channels), F32), jnp.zeros((1, channels), F32)]
    for k in range(2):
        at = pl.ds(k * part, part)
        decays = jnp.exp(decay_ref[at, :])
        d_mixed = dm[at, :]
        d_gate_ref[at, :] = (d_mixed * states[at, :] * slope[at, :]).astype(BF16)
        lane = lax.broadcasted_iota(jnp.int32, decays.shape, 1)
        following = jnp.where(lane < rows - 1, shifted(decays, 1), 1.0)
        products, local = reverse_scan(following, d_mixed * gelu[at, :])
        prod[at, :] = products
        g_step_ref[at, :] = local
        same = lax.broadcasted_iota(jnp.int32, (part, channels), 0) + k * part == lax.broadcasted_iota(
            jnp.int32, (part, channels), 1
        )
        first = decays[:, 0:1]
        for i, ended in enumerate((products, local)):
            lines[i] = lines[i] + jnp.sum(jnp.where(same, first * ended[:, 0:1], 0.0), axis=0, keepdims=True)
    ends[...] = jnp.zeros_like(ends)
    row[...] = jnp.zeros_like(row)
    ends[0:1, :] = lines[0]
    ends[1:2, :] = lines[1]
    ends_x[x] = ends[...]
    passed = []
    for d in range(1, 4):
        copy = remote(ends, ends_x.at[x], e_send.at[d - 1], ex_recv.at[d - 1], z * 4 + lax.rem(x + d, 4), tp)
        copy.start()
        passed.append(copy)

    def cross_sum(t):
        j = order[t]
        total = term[j, x].astype(F32)
        for d in range(1, 4):
            remote(from_x.at[d - 1, j], from_x.at[d - 1, j], x_send.at[t, d - 1], x_recv.at[t, d - 1], sp, mate).wait_recv()
            total = total + from_x[d - 1, j].astype(F32)
        sums[j] = total.astype(BF16)

        @pl.when(j == z)
        def _():
            g_proj_ref[...] = total

        @pl.when(j != z)
        def _():
            remote(sums.at[j], from_z.at[z], z_send.at[j], z_recv.at[z], j * 4 + x, tp).start()

    for t in range(4):
        cross_sum(t)
    scale, shift = jnp.ones((1, channels), F32), jnp.zeros((1, channels), F32)
    for d in range(1, 4):
        q = lax.rem(x + 4 - d, 4)
        remote(ends, ends_x.at[q], e_send.at[d - 1], ex_recv.at[d - 1], sp, mate).wait_recv()
    for q in reversed(range(4)):
        shift = ends_x[q, 1:2, :] + ends_x[q, 0:1, :] * shift
        scale = ends_x[q, 0:1, :] * scale
    row[0:1, :] = scale
    row[1:2, :] = shift
    for d in range(1, 8):
        copy = remote(row, ends_z.at[z], e_send.at[d + 2], ez_recv.at[d - 1], lax.rem(z + d, 8) * 4 + x, tp)
        copy.start()
        passed.append(copy)
    for t in range(4, 8):
        cross_sum(t)
    for d in range(1, 8):
        q = lax.rem(z + 8 - d, 8)
        remote(row, ends_z.at[q], e_send.at[d + 2], ez_recv.at[d - 1], sp, mate).wait_recv()
    ends_z[z] = row[...]
    entering = jnp.zeros((1, channels), F32)
    for q in reversed(range(1, 8)):
        entering = jnp.where(q > z, ends_z[q, 1:2, :] + ends_z[q, 0:1, :] * entering, entering)
    for q in reversed(range(1, 4)):
        entering = jnp.where(q > x, ends_x[q, 1:2, :] + ends_x[q, 0:1, :] * entering, entering)
    for k in range(2):
        at = pl.ds(k * part, part)
        same = lax.broadcasted_iota(jnp.int32, (part, channels), 0) + k * part == lax.broadcasted_iota(
            jnp.int32, (part, channels), 1
        )
        column = jnp.sum(jnp.where(same, entering, 0.0), axis=1, keepdims=True)
        grad = g_step_ref[at, :] + prod[at, :] * column
        g_step_ref[at, :] = grad
        g_log_ref[at, :] = grad * jnp.exp(decay_ref[at, :]) * before_ref[at, :]
    for d in range(1, 8):
        q = lax.rem(z + d, 8)
        remote(from_z.at[q], from_z.at[q], z_send.at[q], z_recv.at[q], sp, mate).wait_recv()
        g_proj_ref[...] += from_z[q].astype(F32)
    for d in range(1, 8):
        q = lax.rem(z + d, 8)
        remote(sums.at[q], from_z.at[z], z_send.at[q], z_recv.at[z], sp, mate).wait_send()
    for copy in sent + crossing + passed:
        copy.wait_send()


def tail(back, pick, cot_t, proj, gate, decay, before, step):
    channels, rows = gate.shape
    depth = cot_t.shape[0]
    flat = (channels, rows)
    lines = 8 * depth // 32
    outs = [(flat, BF16), (flat, F32), (flat, F32), ((lines, channels), F32)]
    dma = pltpu.SemaphoreType.DMA
    return pl.pallas_call(
        tail_kernel,
        in_specs=[pl.BlockSpec(memory_space=VMEM)] * 8,
        out_specs=[pl.BlockSpec(memory_space=VMEM)] * 4,
        out_shape=[jax.ShapeDtypeStruct(s, d) for s, d in outs],
        scratch_shapes=[
            VMEM((8, depth, rows), BF16),
            VMEM((8, 4, lines, channels), BF16),
            VMEM((3, 8, lines, channels), BF16),
            VMEM((8, lines, channels), BF16),
            VMEM((8, lines, channels), BF16),
            VMEM((8, channels), F32),
            VMEM((4, 8, channels), F32),
            VMEM((8, channels), F32),
            VMEM((8, 8, channels), F32),
            VMEM(flat, F32),
            VMEM(flat, F32),
            VMEM(flat, F32),
            VMEM(flat, BF16),
            VMEM(flat, F32),
            VMEM(flat, F32),
            dma((11,)), dma((2,)), dma((2,)), dma((2,)), dma((5,)),
            dma((8, 3)), dma((8, 3)), dma((8,)), dma((8,)), dma((10,)), dma((3,)), dma((7,)),
        ],
        compiler_params=pltpu.CompilerParams(collective_id=1, has_side_effects=True, vmem_limit_bytes=48 << 20),
        name="tail",
    )(back, pick, cot_t, proj, gate, decay, before, step)


N_SENDS = 14
ORDER = (0, 1, 3, 5, 4, 2, 6, 7)
FAR = (2, 5)


def experts_kernel(send_ref, w_gate_ref, w_up_ref, w_down_ref,
                   acc_t, g_down_ref, back_ref,
                   buf, w_cat, w_cat_t, w_down_t, parts, from_mate, pair, from_far, from_left, from_right, ret, back,
                   a_send, a_recv, far_send, far_recv, sends, yl, yr, ya, ym, pm, fa, fl, fr, b_send, b_recv):
    sp, tp, z, x, right, left, across, flip = place()
    mate = tp + flip
    core = lax.rem(tp, 2)
    y = lax.div(tp, 2)
    y_right, y_left, y_far = lax.rem(y + 1, 4), lax.rem(y + 3, 4), lax.rem(y + 2, 4)
    n_sp, both_caps, depth = send_ref.shape[1:]
    cap = both_caps // 2
    n_z = n_sp // 4
    steps = 2 * n_z
    arrive = greet([(lax.rem(sp + k, n_sp), tp) for k in range(1, n_sp)] + [(sp, right), (sp, left), (sp, mate)])

    def dz(i):
        found = 0
        for k, value in enumerate(ORDER):
            found = jnp.where(i == k, value, found)
        return found

    def source(i):
        return lax.rem(z + dz(i), n_z) * 4

    def target(i):
        return lax.rem(z - dz(i) + n_z, n_z) * 4

    def is_far(i):
        return (i >= FAR[0]) & (i < FAR[1])

    def out_copy(i, d):
        to = target(i) + lax.rem(x + d, 4)
        return remote(send_ref.at[0, to], buf.at[tp, sp], a_send.at[i, d], a_recv.at[i, x], to, tp)

    def out_far(i, d):
        to = target(i) + lax.rem(x + d, 4)
        return remote(send_ref.at[1, to], buf.at[across, sp], far_send.at[i, d], far_recv.at[i, x], to, tp)

    def back_copy(i, q):
        to = source(i) + q
        return remote(ret.at[to], back.at[sp], b_send.at[i, q], b_recv.at[i, x], to, tp)

    arrive()
    pltpu.make_async_copy(send_ref.at[0, sp], buf.at[tp, sp], a_recv.at[0, x]).start()
    pltpu.make_async_copy(send_ref.at[1, sp], buf.at[across, sp], far_recv.at[0, x]).start()
    for d in range(1, 4):
        out_copy(0, d).start()
        out_far(0, d).start()

    @pl.loop(1, n_z)
    def _(i):
        for d in range(4):
            out_copy(i, d).start()

        @pl.when(jnp.logical_not(is_far(i)))
        def _():
            for d in range(4):
                out_far(i, d).start()

    def wait(ref, sem):
        remote(ref, ref, a_send.at[0, 0], sem, sp, mate).wait_recv()

    w_cat[:, 0:128] = w_gate_ref[...]
    w_cat[:, 128:256] = w_up_ref[...]
    acc_t[...] = jnp.zeros_like(acc_t)
    g_down_ref[...] = jnp.zeros_like(g_down_ref)

    @pl.loop(0, 8)
    def _(j):
        at = pl.ds(pl.multiple_of(j * depth, depth), depth)
        w_cat_t[:, at] = w_cat[at, :].astype(F32).T.astype(BF16)
        w_down_t[at, :] = w_down_ref[:, at].astype(F32).T.astype(BF16)

    def first(s):
        return source(lax.div(s, 2)) + 2 * lax.rem(s, 2)

    def far(s):
        return is_far(lax.div(s, 2))

    def sends_of(s, *which):
        at = first(s)
        blk = pl.ds(at, 2)

        def same(j, to, k, recv):
            return remote(buf.at[j, blk], buf.at[j, blk], sends.at[s, k], recv, sp, to)

        makers = [
            lambda: same(tp, right, 0, yl.at[s]),
            lambda: same(tp, left, 1, yr.at[s]),
            lambda: same(tp, mate, 2, ym.at[s, 0]),
            lambda: remote(buf.at[left, at], buf.at[left, at], sends.at[s, 3], ya.at[s, 0], sp, right),
            lambda: remote(buf.at[right, at + 1], buf.at[right, at + 1], sends.at[s, 4], ya.at[s, 1], sp, left),
            lambda: same(left, mate, 5, ym.at[s, 1]),
            lambda: same(right, mate, 6, ym.at[s, 2]),
            lambda: same(across, mate, 7, ym.at[s, 3]),
            lambda: remote(parts.at[1 - core, :, blk], from_mate.at[:, blk], sends.at[s, 8], pm.at[s], sp, mate),
            lambda: remote(pair.at[y_far, at], from_far.at[at], sends.at[s, 9], fa.at[s, 0], sp, right),
            lambda: remote(pair.at[y_far, at + 1], from_far.at[at + 1], sends.at[s, 10], fa.at[s, 1], sp, left),
            lambda: remote(pair.at[y_right, blk], from_left.at[blk], sends.at[s, 11], fl.at[s], sp, right),
            lambda: remote(pair.at[y_left, blk], from_right.at[blk], sends.at[s, 12], fr.at[s], sp, left),
        ]
        return [makers[k]() for k in which]

    def start(s, *which):
        for copy in sends_of(s, *which):
            copy.start()

    def spread(s):
        i, q = lax.div(s, 2), 2 * lax.rem(s, 2)
        at = first(s)
        for k in range(2):
            wait(buf.at[tp, at + k], a_recv.at[i, q + k])
        start(s, 0, 1, 2)

        @pl.when(jnp.logical_not(far(s)))
        def _():
            for k in range(2):
                wait(buf.at[across, at + k], far_recv.at[i, q + k])
            start(s, 7)

    def forward(s):
        blk = pl.ds(first(s), 2)
        wait(buf.at[left, blk], yl.at[s])
        wait(buf.at[right, blk], yr.at[s])

        @pl.when(far(s))
        def _():
            start(s, 3, 4)

        start(s, 5, 6)

    def hand_over(s):
        @pl.when(far(s))
        def _():
            wait(buf.at[across, first(s)], ya.at[s, 0])
            wait(buf.at[across, first(s) + 1], ya.at[s, 1])
            start(s, 7)

    def compute(s):
        blk = pl.ds(first(s), 2)
        for k, j in enumerate((tp, left, right, across)):
            wait(buf.at[j + flip, blk], ym.at[s, k])
        size = 2 * cap

        def rows_of(j):
            return buf[j, blk, 0:cap, :].reshape(size, depth)

        def cots_of(j):
            return buf[j, blk, cap : 2 * cap, :].reshape(size, depth)

        act = jnp.zeros((size, 256), F32)
        d_hidden = jnp.zeros((size, 128), F32)
        for j in range(8):
            cols = slice(j * depth, (j + 1) * depth)
            act = act + contract(rows_of(j), w_cat[cols, :], 1, 0)
            d_hidden = d_hidden + contract(cots_of(j), w_down_t[cols, :], 1, 0)
        gate_act, up_act = act[:, 0:128], act[:, 128:256]
        sig = jax.nn.sigmoid(gate_act)
        silu = gate_act * sig
        hidden = (silu * up_act).astype(BF16)
        d_gate = (d_hidden * up_act * (sig * (1.0 + gate_act * (1.0 - sig)))).astype(BF16)
        d_up = (d_hidden * silu).astype(BF16)
        d_both = jnp.concatenate([d_gate, d_up], axis=1)
        d_both_t = d_both.astype(F32).T.astype(BF16)
        hidden_t = hidden.astype(F32).T.astype(BF16)
        for j in range(8):
            cols = slice(j * depth, (j + 1) * depth)
            value = contract(d_both, w_cat_t[:, cols], 1, 0).astype(BF16)
            parts[j % 2, j // 2, blk] = value.reshape(2, cap, depth)
        start(s, 8)
        for j in range(8):
            cols = slice(j * depth, (j + 1) * depth)
            acc_t[:, cols] += contract(d_both_t, rows_of(j), 1, 0)
            g_down_ref[:, cols] += contract(hidden_t, cots_of(j), 1, 0)

    def pair_up(s):
        blk = pl.ds(first(s), 2)
        wait(from_mate.at[:, blk], pm.at[s])
        for k in range(4):
            pair[k, blk] = (parts[core, k, blk].astype(F32) + from_mate[k, blk].astype(F32)).astype(BF16)
        start(s, 9, 10)

    def join(s):
        at = first(s)
        for k, h in ((y_right, 0), (y_left, 1)):
            wait(from_far.at[at + h], fa.at[s, h])
            pair[k, at + h] = (pair[k, at + h].astype(F32) + from_far[at + h].astype(F32)).astype(BF16)
        start(s, 11, 12)

    def finish(s):
        i, q = lax.div(s, 2), 2 * lax.rem(s, 2)
        at = first(s)
        blk = pl.ds(at, 2)
        wait(from_left.at[blk], fl.at[s])
        wait(from_right.at[blk], fr.at[s])
        ret[blk] = (pair[y, blk].astype(F32) + from_left[blk].astype(F32) + from_right[blk].astype(F32)).astype(BF16)
        for k in range(2):
            @pl.when(at + k == sp)
            def _():
                pltpu.make_async_copy(ret.at[sp], back.at[sp], b_recv.at[0, x]).start()

            @pl.when(at + k != sp)
            def _():
                back_copy(i, q + k).start()

    stages = ((spread, 0), (forward, 1), (hand_over, 2), (finish, 6), (join, 5), (pair_up, 4), (compute, 3))

    @pl.loop(0, steps + 6)
    def _(t):
        for stage, late in stages:
            @pl.when((t >= late) & (t < steps + late))
            def _():
                stage(t - late)

    @pl.loop(0, n_z)
    def _(i):
        for q in range(4):
            wait(back.at[target(i) + q], b_recv.at[i, q])

    back_ref[...] = back[...]

    @pl.loop(0, steps)
    def _(s):
        for copy in sends_of(s, 0, 1, 2, 5, 6, 7, 8, 9, 10, 11, 12):
            copy.wait_send()

        @pl.when(far(s))
        def _():
            for copy in sends_of(s, 3, 4):
                copy.wait_send()

    @pl.loop(0, n_z)
    def _(i):
        for d in range(4):
            @pl.when(target(i) + lax.rem(x + d, 4) != sp)
            def _():
                out_copy(i, d).wait_send()

                @pl.when(jnp.logical_not(is_far(i)))
                def _():
                    out_far(i, d).wait_send()

            @pl.when(source(i) + d != sp)
            def _():
                back_copy(i, d).wait_send()


def experts_pass(send, w_gate, w_up, w_down):
    _, n_sp, both_caps, depth = send.shape
    model, units = w_gate.shape
    cap = both_caps // 2
    block = (n_sp, cap, depth)
    n_z = n_sp // 4
    steps = 2 * n_z
    dma = pltpu.SemaphoreType.DMA
    outs = [((2 * units, model), F32), ((units, model), F32), (block, BF16)]
    return pl.pallas_call(
        experts_kernel,
        in_specs=[pl.BlockSpec(memory_space=VMEM)] * 4,
        out_specs=[pl.BlockSpec(memory_space=VMEM)] * 3,
        out_shape=[jax.ShapeDtypeStruct(s, d) for s, d in outs],
        scratch_shapes=[
            VMEM((8, n_sp, both_caps, depth), BF16),
            VMEM((model, 2 * units), BF16),
            VMEM((2 * units, model), BF16),
            VMEM((model, units), BF16),
            VMEM((2, 4, *block), BF16),
            VMEM((4, *block), BF16),
            VMEM((4, *block), BF16),
            VMEM(block, BF16),
            VMEM(block, BF16),
            VMEM(block, BF16),
            VMEM(block, BF16),
            VMEM(block, BF16),
            dma((n_z, 4)), dma((n_z, 4)), dma((n_z, 4)), dma((n_z, 4)), dma((steps, N_SENDS)),
            dma((steps,)), dma((steps,)), dma((steps, 2)), dma((steps, 4)), dma((steps,)), dma((steps, 2)),
            dma((steps,)), dma((steps,)), dma((n_z, 4)), dma((n_z, 4)),
        ],
        compiler_params=pltpu.CompilerParams(collective_id=0, has_side_effects=True, vmem_limit_bytes=60 << 20),
        name="experts",
    )(send, w_gate, w_up, w_down)


def settle_kernel(acc_ref, down_in, gate_in, step_in, log_in, proj_in, g_gate, g_up, g_down, d_gate, g_step, g_log, g_proj):
    both = acc_ref[...].T
    units = g_gate.shape[1]
    g_gate[...] = both[:, 0:units]
    g_up[...] = both[:, units : 2 * units]
    for src, dst in ((down_in, g_down), (gate_in, d_gate), (step_in, g_step), (log_in, g_log), (proj_in, g_proj)):
        dst[...] = src[...]


def settle(acc_t, g_down, d_gate, g_step, g_log, g_proj):
    parts = 4
    units, model = g_down.shape

    def rows(a):
        return pl.BlockSpec((a.shape[0] // parts, a.shape[1]), lambda i: (i, 0))

    def cols(a):
        return pl.BlockSpec((a.shape[0], a.shape[1] // parts), lambda i: (0, i))

    tall = jax.ShapeDtypeStruct((model, units), F32)
    rest = [d_gate, g_step, g_log, g_proj]
    return pl.pallas_call(
        settle_kernel,
        grid=(parts,),
        in_specs=[cols(acc_t), cols(g_down)] + [rows(a) for a in rest],
        out_specs=[rows(tall), rows(tall), cols(g_down)] + [rows(a) for a in rest],
        out_shape=[tall, tall] + [jax.ShapeDtypeStruct(a.shape, a.dtype) for a in [g_down] + rest],
        name="settle",
    )(acc_t, g_down, *rest)


def on_device(resid, cotangent, routes, route_weight, w_gate, w_up, w_down, out_proj, gate_pre, log_decay,
              state_before, step_input):
    rows, model = resid.shape
    experts, n_tp = lax.axis_size("sp"), lax.axis_size("tp")
    cap = 2 * rows * routes.shape[1] // experts
    send, pick, cot_t = front(routes.T, route_weight.T, resid, cotangent, experts, cap, n_tp)
    acc_t, grad_down, back = experts_pass(send, w_gate[0], w_up[0], w_down[0])
    ended = tail(back, pick, cot_t, out_proj.T, gate_pre.T, log_decay.T, state_before.T, step_input.T)
    grad_gate, grad_up, grad_down, d_gate, grad_step, grad_log, grad_proj = settle(acc_t, grad_down, *ended)
    return grad_gate[None], grad_up[None], grad_down[None], grad_proj, d_gate.T, grad_step.T, grad_log.T


def solution(mesh):
    by_sp, both = P("sp", None), P("sp", "tp")
    cols = P("sp", None, "tp")
    return jax.shard_map(
        on_device,
        mesh=mesh,
        in_specs=(by_sp, by_sp, by_sp, by_sp, cols, cols, P("sp", "tp", None), P(None, "tp"), both, both, both, both),
        out_specs=(cols, cols, P("sp", "tp", None), both, both, both, both),
        check_vma=False,
    )
```

```python
import functools
import math

import jax
import jax.numpy as jnp
from jax import lax
from jax.experimental import pallas as pl
from jax.experimental.pallas import tpu as pltpu
from jax.sharding import PartitionSpec as P

F32, BF16 = jnp.float32, jnp.bfloat16
VMEM = pltpu.VMEM
ROOT = math.sqrt(2.0 / math.pi)


def contract(a, b, da, db):
    return lax.dot_general(a, b, (((da,), (db,)), ((), ())), preferred_element_type=F32)


def front_kernel(experts, cap, tp_ref, routes_ref, weight_ref, resid_ref, cot_ref, resid_far_ref, cot_far_ref,
                 send_ref, pick_ref, cot_t_ref):
    rows = routes_ref.shape[1]
    width = resid_ref.shape[1]
    r0, r1 = routes_ref[0:1, :], routes_ref[1:2, :]
    w0, w1 = weight_ref[0:1, :], weight_ref[1:2, :]
    ids = lax.broadcasted_iota(jnp.int32, (experts, rows), 0)
    is0, is1 = ids == r0, ids == r1
    named = (jnp.where(is0, 1.0, 0.0) + jnp.where(is1, 1.0, 0.0)).astype(BF16)
    before = lax.broadcasted_iota(jnp.int32, (rows, rows), 0) < lax.broadcasted_iota(jnp.int32, (rows, rows), 1)
    counts = contract(named, jnp.where(before, 1.0, 0.0).astype(BF16), 1, 0)
    slot0 = r0 * cap + jnp.sum(jnp.where(is0, counts, 0.0), axis=0, keepdims=True).astype(jnp.int32)
    slot1 = r1 * cap + jnp.sum(jnp.where(is1, counts, 0.0), axis=0, keepdims=True).astype(jnp.int32)
    part = 8
    for k in range(experts // part):
        size = part * cap
        at = lax.broadcasted_iota(jnp.int32, (size, rows), 0) + k * size
        p0, p1 = at == slot0, at == slot1
        pick = (jnp.where(p0, 1.0, 0.0) + jnp.where(p1, 1.0, 0.0)).astype(BF16)
        pick_ref[k * size : (k + 1) * size, :] = pick
        scale = jnp.sum(jnp.where(p0, w0, 0.0) + jnp.where(p1, w1, 0.0), axis=1, keepdims=True)
        at = slice(k * part, (k + 1) * part)
        for i, (resid, cot) in enumerate(((resid_ref, cot_ref), (resid_far_ref, cot_far_ref))):
            got = contract(pick, resid[...], 1, 0).astype(BF16)
            cots = (scale * contract(pick, cot[...], 1, 0)).astype(BF16)
            send_ref[i, at, 0:cap, :] = got.reshape(part, cap, width)
            send_ref[i, at, cap : 2 * cap, :] = cots.reshape(part, cap, width)
    cot_t_ref[...] = cot_ref[...].astype(F32).T.astype(BF16)


def front(routes_t, weight_t, resid, cotangent, experts, cap, n_tp):
    rows, model = resid.shape
    width = model // n_tp
    tp = lax.axis_index("tp").astype(jnp.int32)
    slices = jnp.stack([tp, lax.rem(tp + n_tp // 2, n_tp)])
    whole = lambda shape: pl.BlockSpec(shape, lambda i, t: (0,) * len(shape))
    cols = pl.BlockSpec((rows, width), lambda i, t: (0, t[0]))
    far = pl.BlockSpec((rows, width), lambda i, t: (0, t[1]))
    return pl.pallas_call(
        functools.partial(front_kernel, experts, cap),
        grid_spec=pltpu.PrefetchScalarGridSpec(
            num_scalar_prefetch=1,
            grid=(1,),
            in_specs=[whole((2, rows)), whole((2, rows)), cols, cols, far, far],
            out_specs=[whole((2, experts, 2 * cap, width)), whole((experts * cap, rows)), whole((width, rows))],
        ),
        out_shape=[
            jax.ShapeDtypeStruct((2, experts, 2 * cap, width), BF16),
            jax.ShapeDtypeStruct((experts * cap, rows), BF16),
            jax.ShapeDtypeStruct((width, rows), BF16),
        ],
        compiler_params=pltpu.CompilerParams(vmem_limit_bytes=24 << 20),
        name="front",
    )(slices, routes_t, weight_t, resid, cotangent, resid, cotangent)


def shifted(x, by):
    return pltpu.roll(x, x.shape[1] - by, 1)


def reverse_scan(factor, value):
    rows = factor.shape[1]
    lane = lax.broadcasted_iota(jnp.int32, factor.shape, 1)
    by = 1
    while by < rows:
        inside = lane < rows - by
        value = value + factor * jnp.where(inside, shifted(value, by), 0.0)
        factor = factor * jnp.where(inside, shifted(factor, by), 1.0)
        by *= 2
    return factor, value


MESH = pl.DeviceIdType.MESH


def place():
    sp, tp = lax.axis_index("sp"), lax.axis_index("tp")
    z, x, core = lax.div(sp, 4), lax.rem(sp, 4), lax.rem(tp, 2)
    right, left, across = lax.rem(tp + 2, 8), lax.rem(tp + 6, 8), lax.rem(tp + 4, 8)
    return sp, tp, z, x, right, left, across, 1 - 2 * core


def remote(src, dst, send, recv, sp, tp):
    return pltpu.make_async_remote_copy(
        src_ref=src, dst_ref=dst, send_sem=send, recv_sem=recv, device_id={"sp": sp, "tp": tp}, device_id_type=MESH
    )


def greet(peers):
    barrier = pltpu.get_barrier_semaphore()
    for sp, tp in peers:
        pl.semaphore_signal(barrier, inc=1, device_id={"sp": sp, "tp": tp}, device_id_type=MESH)
    return lambda: pl.semaphore_wait(barrier, len(peers))


def tail_kernel(back_ref, pick_ref, cot_t_ref, proj_ref, gate_ref, decay_ref, before_ref, step_ref,
                d_gate_ref, g_step_ref, g_log_ref, g_proj_ref,
                rg, term, from_x, sums, from_z, ends, ends_x, row, ends_z, states, gelu, slope, mixed, dm, prod,
                ag_send, ag_l, ag_r, ag_a, ag_d, x_send, x_recv, z_send, z_recv, e_send, ex_recv, ez_recv):
    sp, tp, z, x, right, left, across, flip = place()
    mate = tp + flip
    channels, rows = gate_ref.shape
    depth = rg.shape[1]
    half_rows = depth // 2
    part = channels // 2
    xs = [z * 4 + lax.rem(x + d, 4) for d in range(1, 4)]
    zs = [lax.rem(z + d, 8) * 4 + x for d in range(1, 8)]
    arrive = greet([(sp, right), (sp, left), (sp, mate)] + [(q, tp) for q in xs + zs])

    slots = pick_ref.shape[0]
    routed = contract(back_ref[...].reshape(slots, depth), pick_ref[...], 0, 0)
    rg[tp] = (cot_t_ref[...].astype(F32) + routed).astype(BF16)
    arrive()

    def half(j, h):
        return rg.at[j, pl.ds(h * half_rows, half_rows), :]

    def moved(ref, k, recv, to):
        return remote(ref, ref, ag_send.at[k], recv, sp, to)

    sent = [
        moved(half(tp, 0), 0, ag_l.at[0], right),
        moved(half(tp, 1), 1, ag_r.at[1], left),
        moved(half(tp, 1), 2, ag_l.at[1], right),
        moved(half(tp, 0), 3, ag_r.at[0], left),
        moved(rg.at[tp], 4, ag_d.at[0], mate),
    ]
    for copy in sent:
        copy.start()

    def prepare(k):
        at = pl.ds(k * part, part)
        v = gate_ref[at, :].astype(F32)
        decays = jnp.exp(decay_ref[at, :])
        state = decays * before_ref[at, :] + step_ref[at, :].astype(F32)
        th = jnp.tanh(ROOT * (v + 0.044715 * (v * v * v)))
        act = 0.5 * v * (1.0 + th)
        gelu[at, :] = act
        states[at, :] = state
        slope[at, :] = 0.5 * (1.0 + th) + 0.5 * v * (1.0 - th * th) * (ROOT * (1.0 + 3.0 * 0.044715 * (v * v)))
        mixed[at, :] = (act * state).astype(BF16)

    def pass_on(ref, k, arrived, recv, to):
        moved(ref, k, arrived, to).wait_recv()
        copy = moved(ref, k, recv, to)
        copy.start()
        sent.append(copy)

    prepare(0)
    pass_on(half(left, 0), 5, ag_l.at[0], ag_a.at[0], right)
    pass_on(half(right, 1), 6, ag_r.at[1], ag_a.at[1], left)
    prepare(1)

    crossing = []

    def use(t, j):
        cols = pl.ds(pl.multiple_of(j * depth, depth), depth)
        piece = rg[j]
        term[j] = contract(piece, mixed[...], 1, 1).astype(BF16).reshape(term.shape[1:])
        for d in range(1, 4):
            to = lax.rem(x + d, 4)
            copy = remote(term.at[j, to], from_x.at[d - 1, j], x_send.at[t, d - 1], x_recv.at[t, d - 1], z * 4 + to, tp)
            copy.start()
            crossing.append(copy)
        product = contract(proj_ref[:, cols], piece, 1, 0)
        dm[...] = product if t == 0 else dm[...] + product

    use(0, tp)
    moved(rg.at[mate], 4, ag_d.at[0], mate).wait_recv()
    use(1, mate)
    moved(half(left, 1), 7, ag_l.at[1], mate).wait_recv()
    copy = moved(rg.at[left], 7, ag_d.at[1], mate)
    copy.start()
    sent.append(copy)
    moved(half(right, 0), 8, ag_r.at[0], mate).wait_recv()
    copy = moved(rg.at[right], 8, ag_d.at[2], mate)
    copy.start()
    sent.append(copy)
    use(2, left)
    use(3, right)
    pass_on(half(across, 0), 9, ag_a.at[0], ag_d.at[3], mate)
    pass_on(half(across, 1), 10, ag_a.at[1], ag_d.at[4], mate)
    moved(rg.at[left + flip], 7, ag_d.at[1], mate).wait_recv()
    use(4, left + flip)
    moved(rg.at[right + flip], 8, ag_d.at[2], mate).wait_recv()
    use(5, right + flip)
    use(6, across)
    moved(half(across + flip, 0), 9, ag_d.at[3], mate).wait_recv()
    moved(half(across + flip, 1), 10, ag_d.at[4], mate).wait_recv()
    use(7, across + flip)
    order = [tp, mate, left, right, left + flip, right + flip, across, across + flip]

    lines = [jnp.zeros((1, channels), F32), jnp.zeros((1, channels), F32)]
    for k in range(2):
        at = pl.ds(k * part, part)
        decays = jnp.exp(decay_ref[at, :])
        d_mixed = dm[at, :]
        d_gate_ref[at, :] = (d_mixed * states[at, :] * slope[at, :]).astype(BF16)
        lane = lax.broadcasted_iota(jnp.int32, decays.shape, 1)
        following = jnp.where(lane < rows - 1, shifted(decays, 1), 1.0)
        products, local = reverse_scan(following, d_mixed * gelu[at, :])
        prod[at, :] = products
        g_step_ref[at, :] = local
        same = lax.broadcasted_iota(jnp.int32, (part, channels), 0) + k * part == lax.broadcasted_iota(
            jnp.int32, (part, channels), 1
        )
        first = decays[:, 0:1]
        for i, ended in enumerate((products, local)):
            lines[i] = lines[i] + jnp.sum(jnp.where(same, first * ended[:, 0:1], 0.0), axis=0, keepdims=True)
    ends[...] = jnp.zeros_like(ends)
    row[...] = jnp.zeros_like(row)
    ends[0:1, :] = lines[0]
    ends[1:2, :] = lines[1]
    ends_x[x] = ends[...]
    passed = []
    for d in range(1, 4):
        copy = remote(ends, ends_x.at[x], e_send.at[d - 1], ex_recv.at[d - 1], z * 4 + lax.rem(x + d, 4), tp)
        copy.start()
        passed.append(copy)

    def cross_sum(t):
        j = order[t]
        total = term[j, x].astype(F32)
        for d in range(1, 4):
            remote(from_x.at[d - 1, j], from_x.at[d - 1, j], x_send.at[t, d - 1], x_recv.at[t, d - 1], sp, mate).wait_recv()
            total = total + from_x[d - 1, j].astype(F32)
        sums[j] = total.astype(BF16)

        @pl.when(j == z)
        def _():
            g_proj_ref[...] = total

        @pl.when(j != z)
        def _():
            remote(sums.at[j], from_z.at[z], z_send.at[j], z_recv.at[z], j * 4 + x, tp).start()

    for t in range(4):
        cross_sum(t)
    scale, shift = jnp.ones((1, channels), F32), jnp.zeros((1, channels), F32)
    for d in range(1, 4):
        q = lax.rem(x + 4 - d, 4)
        remote(ends, ends_x.at[q], e_send.at[d - 1], ex_recv.at[d - 1], sp, mate).wait_recv()
    for q in reversed(range(4)):
        shift = ends_x[q, 1:2, :] + ends_x[q, 0:1, :] * shift
        scale = ends_x[q, 0:1, :] * scale
    row[0:1, :] = scale
    row[1:2, :] = shift
    for d in range(1, 8):
        copy = remote(row, ends_z.at[z], e_send.at[d + 2], ez_recv.at[d - 1], lax.rem(z + d, 8) * 4 + x, tp)
        copy.start()
        passed.append(copy)
    for t in range(4, 8):
        cross_sum(t)
    for d in range(1, 8):
        q = lax.rem(z + 8 - d, 8)
        remote(row, ends_z.at[q], e_send.at[d + 2], ez_recv.at[d - 1], sp, mate).wait_recv()
    ends_z[z] = row[...]
    entering = jnp.zeros((1, channels), F32)
    for q in reversed(range(1, 8)):
        entering = jnp.where(q > z, ends_z[q, 1:2, :] + ends_z[q, 0:1, :] * entering, entering)
    for q in reversed(range(1, 4)):
        entering = jnp.where(q > x, ends_x[q, 1:2, :] + ends_x[q, 0:1, :] * entering, entering)
    for k in range(2):
        at = pl.ds(k * part, part)
        same = lax.broadcasted_iota(jnp.int32, (part, channels), 0) + k * part == lax.broadcasted_iota(
            jnp.int32, (part, channels), 1
        )
        column = jnp.sum(jnp.where(same, entering, 0.0), axis=1, keepdims=True)
        grad = g_step_ref[at, :] + prod[at, :] * column
        g_step_ref[at, :] = grad
        g_log_ref[at, :] = grad * jnp.exp(decay_ref[at, :]) * before_ref[at, :]
    for d in range(1, 8):
        q = lax.rem(z + d, 8)
        remote(from_z.at[q], from_z.at[q], z_send.at[q], z_recv.at[q], sp, mate).wait_recv()
        g_proj_ref[...] += from_z[q].astype(F32)
    for d in range(1, 8):
        q = lax.rem(z + d, 8)
        remote(sums.at[q], from_z.at[z], z_send.at[q], z_recv.at[z], sp, mate).wait_send()
    for copy in sent + crossing + passed:
        copy.wait_send()


def tail(back, pick, cot_t, proj, gate, decay, before, step):
    channels, rows = gate.shape
    depth = cot_t.shape[0]
    flat = (channels, rows)
    lines = 8 * depth // 32
    outs = [(flat, BF16), (flat, F32), (flat, F32), ((lines, channels), F32)]
    dma = pltpu.SemaphoreType.DMA
    return pl.pallas_call(
        tail_kernel,
        in_specs=[pl.BlockSpec(memory_space=VMEM)] * 8,
        out_specs=[pl.BlockSpec(memory_space=VMEM)] * 4,
        out_shape=[jax.ShapeDtypeStruct(s, d) for s, d in outs],
        scratch_shapes=[
            VMEM((8, depth, rows), BF16),
            VMEM((8, 4, lines, channels), BF16),
            VMEM((3, 8, lines, channels), BF16),
            VMEM((8, lines, channels), BF16),
            VMEM((8, lines, channels), BF16),
            VMEM((8, channels), F32),
            VMEM((4, 8, channels), F32),
            VMEM((8, channels), F32),
            VMEM((8, 8, channels), F32),
            VMEM(flat, F32),
            VMEM(flat, F32),
            VMEM(flat, F32),
            VMEM(flat, BF16),
            VMEM(flat, F32),
            VMEM(flat, F32),
            dma((11,)), dma((2,)), dma((2,)), dma((2,)), dma((5,)),
            dma((8, 3)), dma((8, 3)), dma((8,)), dma((8,)), dma((10,)), dma((3,)), dma((7,)),
        ],
        compiler_params=pltpu.CompilerParams(collective_id=1, has_side_effects=True, vmem_limit_bytes=24 << 20),
        name="tail",
    )(back, pick, cot_t, proj, gate, decay, before, step)


N_SENDS = 14
ORDER = (0, 1, 3, 5, 4, 2, 6, 7)
FAR = (2, 5)


def experts_kernel(send_ref, w_gate_ref, w_up_ref, w_down_ref,
                   g_gate_ref, g_up_ref, g_down_ref, back_ref,
                   buf, w_cat, w_cat_t, w_down, w_down_t, acc_t, acc_down, g_tall, loads, stores, parts, from_mate, pair, from_far, from_left, from_right, ret, back,
                   a_send, a_recv, far_send, far_recv, sends, yl, yr, ya, ym, pm, fa, fl, fr, b_send, b_recv):
    sp, tp, z, x, right, left, across, flip = place()
    mate = tp + flip
    core = lax.rem(tp, 2)
    y = lax.div(tp, 2)
    y_right, y_left, y_far = lax.rem(y + 1, 4), lax.rem(y + 3, 4), lax.rem(y + 2, 4)
    n_sp, both_caps, depth = send_ref.shape[1:]
    cap = both_caps // 2
    n_z = n_sp // 4
    steps = 2 * n_z
    arrive = greet([(lax.rem(sp + k, n_sp), tp) for k in range(1, n_sp)] + [(sp, right), (sp, left), (sp, mate)])

    def dz(i):
        found = 0
        for k, value in enumerate(ORDER):
            found = jnp.where(i == k, value, found)
        return found

    def source(i):
        return lax.rem(z + dz(i), n_z) * 4

    def target(i):
        return lax.rem(z - dz(i) + n_z, n_z) * 4

    def is_far(i):
        return (i >= FAR[0]) & (i < FAR[1])

    def out_copy(i, d):
        to = target(i) + lax.rem(x + d, 4)
        return remote(send_ref.at[0, to], buf.at[tp, sp], a_send.at[i, d], a_recv.at[i, x], to, tp)

    def out_far(i, d):
        to = target(i) + lax.rem(x + d, 4)
        return remote(send_ref.at[1, to], buf.at[across, sp], far_send.at[i, d], far_recv.at[i, x], to, tp)

    def back_copy(i, q):
        to = source(i) + q
        return remote(ret.at[to], back.at[sp], b_send.at[i, q], b_recv.at[i, x], to, tp)

    weights = [
        pltpu.make_async_copy(w_gate_ref, w_cat.at[:, 0:128], loads.at[0]),
        pltpu.make_async_copy(w_up_ref, w_cat.at[:, 128:256], loads.at[1]),
        pltpu.make_async_copy(w_down_ref, w_down, loads.at[2]),
    ]
    arrive()
    pltpu.make_async_copy(send_ref.at[0, sp], buf.at[tp, sp], a_recv.at[0, x]).start()
    pltpu.make_async_copy(send_ref.at[1, sp], buf.at[across, sp], far_recv.at[0, x]).start()
    for d in range(1, 4):
        out_copy(0, d).start()
        out_far(0, d).start()

    @pl.loop(1, n_z)
    def _(i):
        for d in range(4):
            out_copy(i, d).start()

        @pl.when(jnp.logical_not(is_far(i)))
        def _():
            for d in range(4):
                out_far(i, d).start()

    def wait(ref, sem):
        remote(ref, ref, a_send.at[0, 0], sem, sp, mate).wait_recv()

    for copy in weights:
        copy.start()

    def prepare(t):
        @pl.when(t == 0)
        def _():
            for copy in weights:
                copy.wait()
            acc_t[...] = jnp.zeros_like(acc_t)
            acc_down[...] = jnp.zeros_like(acc_down)

        for k in range(2):
            at = pl.ds(pl.multiple_of((2 * t + k) * depth, depth), depth)
            w_cat_t[:, at] = w_cat[at, :].astype(F32).T.astype(BF16)
            w_down_t[at, :] = w_down[:, at].astype(F32).T.astype(BF16)

    def first(s):
        return source(lax.div(s, 2)) + 2 * lax.rem(s, 2)

    def far(s):
        return is_far(lax.div(s, 2))

    def sends_of(s, *which):
        at = first(s)
        blk = pl.ds(at, 2)

        def same(j, to, k, recv):
            return remote(buf.at[j, blk], buf.at[j, blk], sends.at[s, k], recv, sp, to)

        makers = [
            lambda: same(tp, right, 0, yl.at[s]),
            lambda: same(tp, left, 1, yr.at[s]),
            lambda: same(tp, mate, 2, ym.at[s, 0]),
            lambda: remote(buf.at[left, at], buf.at[left, at], sends.at[s, 3], ya.at[s, 0], sp, right),
            lambda: remote(buf.at[right, at + 1], buf.at[right, at + 1], sends.at[s, 4], ya.at[s, 1], sp, left),
            lambda: same(left, mate, 5, ym.at[s, 1]),
            lambda: same(right, mate, 6, ym.at[s, 2]),
            lambda: same(across, mate, 7, ym.at[s, 3]),
            lambda: remote(parts.at[1 - core, :, blk], from_mate.at[:, blk], sends.at[s, 8], pm.at[s], sp, mate),
            lambda: remote(pair.at[y_far, at], from_far.at[at], sends.at[s, 9], fa.at[s, 0], sp, right),
            lambda: remote(pair.at[y_far, at + 1], from_far.at[at + 1], sends.at[s, 10], fa.at[s, 1], sp, left),
            lambda: remote(pair.at[y_right, blk], from_left.at[blk], sends.at[s, 11], fl.at[s], sp, right),
            lambda: remote(pair.at[y_left, blk], from_right.at[blk], sends.at[s, 12], fr.at[s], sp, left),
        ]
        return [makers[k]() for k in which]

    def start(s, *which):
        for copy in sends_of(s, *which):
            copy.start()

    def spread(s):
        i, q = lax.div(s, 2), 2 * lax.rem(s, 2)
        at = first(s)
        for k in range(2):
            wait(buf.at[tp, at + k], a_recv.at[i, q + k])
        start(s, 0, 1, 2)

        @pl.when(jnp.logical_not(far(s)))
        def _():
            for k in range(2):
                wait(buf.at[across, at + k], far_recv.at[i, q + k])
            start(s, 7)

    def forward(s):
        blk = pl.ds(first(s), 2)
        wait(buf.at[left, blk], yl.at[s])
        wait(buf.at[right, blk], yr.at[s])

        @pl.when(far(s))
        def _():
            start(s, 3, 4)

        start(s, 5, 6)

    def hand_over(s):
        @pl.when(far(s))
        def _():
            wait(buf.at[across, first(s)], ya.at[s, 0])
            wait(buf.at[across, first(s) + 1], ya.at[s, 1])
            start(s, 7)

    def compute(s):
        blk = pl.ds(first(s), 2)
        for k, j in enumerate((tp, left, right, across)):
            wait(buf.at[j + flip, blk], ym.at[s, k])
        size = 2 * cap

        def rows_of(j):
            return buf[j, blk, 0:cap, :].reshape(size, depth)

        def cots_of(j):
            return buf[j, blk, cap : 2 * cap, :].reshape(size, depth)

        act = jnp.zeros((size, 256), F32)
        d_hidden = jnp.zeros((size, 128), F32)
        for j in range(8):
            cols = slice(j * depth, (j + 1) * depth)
            act = act + contract(rows_of(j), w_cat[cols, :], 1, 0)
            d_hidden = d_hidden + contract(cots_of(j), w_down_t[cols, :], 1, 0)
        gate_act, up_act = act[:, 0:128], act[:, 128:256]
        sig = jax.nn.sigmoid(gate_act)
        silu = gate_act * sig
        hidden = (silu * up_act).astype(BF16)
        d_gate = (d_hidden * up_act * (sig * (1.0 + gate_act * (1.0 - sig)))).astype(BF16)
        d_up = (d_hidden * silu).astype(BF16)
        d_both = jnp.concatenate([d_gate, d_up], axis=1)
        d_both_t = d_both.astype(F32).T.astype(BF16)
        hidden_t = hidden.astype(F32).T.astype(BF16)
        for j in range(8):
            cols = slice(j * depth, (j + 1) * depth)
            value = contract(d_both, w_cat_t[:, cols], 1, 0).astype(BF16)
            parts[j % 2, j // 2, blk] = value.reshape(2, cap, depth)
        start(s, 8)
        for j in range(8):
            cols = slice(j * depth, (j + 1) * depth)
            acc_t[:, cols] += contract(d_both_t, rows_of(j), 1, 0)
            acc_down[:, cols] += contract(hidden_t, cots_of(j), 1, 0)

    def pair_up(s):
        blk = pl.ds(first(s), 2)
        wait(from_mate.at[:, blk], pm.at[s])
        for k in range(4):
            pair[k, blk] = (parts[core, k, blk].astype(F32) + from_mate[k, blk].astype(F32)).astype(BF16)
        start(s, 9, 10)

    def join(s):
        at = first(s)
        for k, h in ((y_right, 0), (y_left, 1)):
            wait(from_far.at[at + h], fa.at[s, h])
            pair[k, at + h] = (pair[k, at + h].astype(F32) + from_far[at + h].astype(F32)).astype(BF16)
        start(s, 11, 12)

    def finish(s):
        i, q = lax.div(s, 2), 2 * lax.rem(s, 2)
        at = first(s)
        blk = pl.ds(at, 2)
        wait(from_left.at[blk], fl.at[s])
        wait(from_right.at[blk], fr.at[s])
        ret[blk] = (pair[y, blk].astype(F32) + from_left[blk].astype(F32) + from_right[blk].astype(F32)).astype(BF16)
        for k in range(2):
            @pl.when(at + k == sp)
            def _():
                pltpu.make_async_copy(ret.at[sp], back.at[sp], b_recv.at[0, x]).start()

            @pl.when(at + k != sp)
            def _():
                back_copy(i, q + k).start()

    stages = ((spread, 0), (forward, 2), (hand_over, 4), (finish, 10), (join, 8), (pair_up, 6), (compute, 5))

    @pl.loop(0, steps + 10)
    def _(t):
        for stage, late in stages:
            @pl.when((t >= late) & (t < steps + late))
            def _():
                stage(t - late)

        @pl.when(t < 4)
        def _():
            prepare(t)

    for j in range(8):
        cols = slice(j * depth, (j + 1) * depth)
        both = acc_t[:, cols].T
        g_tall[0, cols, :] = both[:, 0:128]
        g_tall[1, cols, :] = both[:, 128:256]
    results = [
        pltpu.make_async_copy(g_tall.at[0], g_gate_ref, stores.at[0]),
        pltpu.make_async_copy(g_tall.at[1], g_up_ref, stores.at[1]),
        pltpu.make_async_copy(acc_down, g_down_ref, stores.at[2]),
    ]
    for copy in results:
        copy.start()

    @pl.loop(0, n_z)
    def _(i):
        for q in range(4):
            wait(back.at[target(i) + q], b_recv.at[i, q])

    back_ref[...] = back[...]
    for copy in results:
        copy.wait()

    @pl.loop(0, steps)
    def _(s):
        for copy in sends_of(s, 0, 1, 2, 5, 6, 7, 8, 9, 10, 11, 12):
            copy.wait_send()

        @pl.when(far(s))
        def _():
            for copy in sends_of(s, 3, 4):
                copy.wait_send()

    @pl.loop(0, n_z)
    def _(i):
        for d in range(4):
            @pl.when(target(i) + lax.rem(x + d, 4) != sp)
            def _():
                out_copy(i, d).wait_send()

                @pl.when(jnp.logical_not(is_far(i)))
                def _():
                    out_far(i, d).wait_send()

            @pl.when(source(i) + d != sp)
            def _():
                back_copy(i, d).wait_send()


def experts_pass(send, w_gate, w_up, w_down):
    _, n_sp, both_caps, depth = send.shape
    model, units = w_gate.shape
    cap = both_caps // 2
    block = (n_sp, cap, depth)
    n_z = n_sp // 4
    steps = 2 * n_z
    dma = pltpu.SemaphoreType.DMA
    outs = [((model, units), F32), ((model, units), F32), ((units, model), F32), (block, BF16)]
    return pl.pallas_call(
        experts_kernel,
        in_specs=[pl.BlockSpec(memory_space=pl.ANY)] * 4,
        out_specs=[pl.BlockSpec(memory_space=pl.ANY)] * 3 + [pl.BlockSpec(memory_space=VMEM)],
        out_shape=[jax.ShapeDtypeStruct(s, d) for s, d in outs],
        scratch_shapes=[
            VMEM((8, n_sp, both_caps, depth), BF16),
            VMEM((model, 2 * units), BF16),
            VMEM((2 * units, model), BF16),
            VMEM((units, model), BF16),
            VMEM((model, units), BF16),
            VMEM((2 * units, model), F32),
            VMEM((units, model), F32),
            VMEM((2, model, units), F32),
            dma((3,)), dma((3,)),
            VMEM((2, 4, *block), BF16),
            VMEM((4, *block), BF16),
            VMEM((4, *block), BF16),
            VMEM(block, BF16),
            VMEM(block, BF16),
            VMEM(block, BF16),
            VMEM(block, BF16),
            VMEM(block, BF16),
            dma((n_z, 4)), dma((n_z, 4)), dma((n_z, 4)), dma((n_z, 4)), dma((steps, N_SENDS)),
            dma((steps,)), dma((steps,)), dma((steps, 2)), dma((steps, 4)), dma((steps,)), dma((steps, 2)),
            dma((steps,)), dma((steps,)), dma((n_z, 4)), dma((n_z, 4)),
        ],
        compiler_params=pltpu.CompilerParams(collective_id=0, has_side_effects=True, vmem_limit_bytes=44 << 20),
        name="experts",
    )(send, w_gate, w_up, w_down)


def settle_kernel(*refs):
    n = len(refs) // 2
    copies = [pltpu.make_async_copy(refs[k], refs[n + k], refs[2 * n].at[k]) for k in range(n)]
    for copy in copies:
        copy.start()
    for copy in copies:
        copy.wait()


def settle(*values):
    return pl.pallas_call(
        settle_kernel,
        in_specs=[pl.BlockSpec(memory_space=VMEM)] * len(values),
        out_specs=[pl.BlockSpec(memory_space=pl.ANY)] * len(values),
        out_shape=[jax.ShapeDtypeStruct(a.shape, a.dtype) for a in values],
        scratch_shapes=[pltpu.SemaphoreType.DMA((len(values),))],
        compiler_params=pltpu.CompilerParams(vmem_limit_bytes=16 << 20),
        name="settle",
    )(*values)


def on_device(resid, cotangent, routes, route_weight, w_gate, w_up, w_down, out_proj, gate_pre, log_decay,
              state_before, step_input):
    rows, model = resid.shape
    experts, n_tp = lax.axis_size("sp"), lax.axis_size("tp")
    cap = 2 * rows * routes.shape[1] // experts
    send, pick, cot_t = front(routes.T, route_weight.T, resid, cotangent, experts, cap, n_tp)
    grads = experts_pass(send, w_gate[0], w_up[0], w_down[0])
    ended = tail(grads[3], pick, cot_t, out_proj.T, gate_pre.T, log_decay.T, state_before.T, step_input.T)
    grad_gate, grad_up, grad_down, d_gate, grad_step, grad_log, grad_proj = settle(*grads[:3], *ended)
    return grad_gate[None], grad_up[None], grad_down[None], grad_proj, d_gate.T, grad_step.T, grad_log.T


def solution(mesh):
    by_sp, both = P("sp", None), P("sp", "tp")
    cols = P("sp", None, "tp")
    return jax.shard_map(
        on_device,
        mesh=mesh,
        in_specs=(by_sp, by_sp, by_sp, by_sp, cols, cols, P("sp", "tp", None), P(None, "tp"), both, both, both, both),
        out_specs=(cols, cols, P("sp", "tp", None), both, both, both, both),
        check_vma=False,
    )
```

```python
import functools
import math

import jax
import jax.numpy as jnp
from jax import lax
from jax.experimental import pallas as pl
from jax.experimental.pallas import tpu as pltpu
from jax.sharding import PartitionSpec as P

F32, BF16 = jnp.float32, jnp.bfloat16
VMEM = pltpu.VMEM
ROOT = math.sqrt(2.0 / math.pi)


def contract(a, b, da, db):
    return lax.dot_general(a, b, (((da,), (db,)), ((), ())), preferred_element_type=F32)


def front_kernel(experts, cap, tp_ref, routes_ref, weight_ref, resid_ref, cot_ref, resid_far_ref, cot_far_ref,
                 send_ref, pick_ref, cot_t_ref):
    rows = routes_ref.shape[1]
    width = resid_ref.shape[1]
    r0, r1 = routes_ref[0:1, :], routes_ref[1:2, :]
    w0, w1 = weight_ref[0:1, :], weight_ref[1:2, :]
    ids = lax.broadcasted_iota(jnp.int32, (experts, rows), 0)
    is0, is1 = ids == r0, ids == r1
    named = (jnp.where(is0, 1.0, 0.0) + jnp.where(is1, 1.0, 0.0)).astype(BF16)
    before = lax.broadcasted_iota(jnp.int32, (rows, rows), 0) < lax.broadcasted_iota(jnp.int32, (rows, rows), 1)
    counts = contract(named, jnp.where(before, 1.0, 0.0).astype(BF16), 1, 0)
    slot0 = r0 * cap + jnp.sum(jnp.where(is0, counts, 0.0), axis=0, keepdims=True).astype(jnp.int32)
    slot1 = r1 * cap + jnp.sum(jnp.where(is1, counts, 0.0), axis=0, keepdims=True).astype(jnp.int32)
    part = 8
    for k in range(experts // part):
        size = part * cap
        at = lax.broadcasted_iota(jnp.int32, (size, rows), 0) + k * size
        p0, p1 = at == slot0, at == slot1
        pick = (jnp.where(p0, 1.0, 0.0) + jnp.where(p1, 1.0, 0.0)).astype(BF16)
        pick_ref[k * size : (k + 1) * size, :] = pick
        scale = jnp.sum(jnp.where(p0, w0, 0.0) + jnp.where(p1, w1, 0.0), axis=1, keepdims=True)
        at = slice(k * part, (k + 1) * part)
        for i, (resid, cot) in enumerate(((resid_ref, cot_ref), (resid_far_ref, cot_far_ref))):
            got = contract(pick, resid[...], 1, 0).astype(BF16)
            cots = (scale * contract(pick, cot[...], 1, 0)).astype(BF16)
            send_ref[i, at, 0:cap, :] = got.reshape(part, cap, width)
            send_ref[i, at, cap : 2 * cap, :] = cots.reshape(part, cap, width)
    cot_t_ref[...] = cot_ref[...].astype(F32).T.astype(BF16)


def front(routes_t, weight_t, resid, cotangent, experts, cap, n_tp):
    rows, model = resid.shape
    width = model // n_tp
    tp = lax.axis_index("tp").astype(jnp.int32)
    slices = jnp.stack([tp, lax.rem(tp + n_tp // 2, n_tp)])
    whole = lambda shape: pl.BlockSpec(shape, lambda i, t: (0,) * len(shape))
    cols = pl.BlockSpec((rows, width), lambda i, t: (0, t[0]))
    far = pl.BlockSpec((rows, width), lambda i, t: (0, t[1]))
    return pl.pallas_call(
        functools.partial(front_kernel, experts, cap),
        grid_spec=pltpu.PrefetchScalarGridSpec(
            num_scalar_prefetch=1,
            grid=(1,),
            in_specs=[whole((2, rows)), whole((2, rows)), cols, cols, far, far],
            out_specs=[whole((2, experts, 2 * cap, width)), whole((experts * cap, rows)), whole((width, rows))],
        ),
        out_shape=[
            jax.ShapeDtypeStruct((2, experts, 2 * cap, width), BF16),
            jax.ShapeDtypeStruct((experts * cap, rows), BF16),
            jax.ShapeDtypeStruct((width, rows), BF16),
        ],
        compiler_params=pltpu.CompilerParams(vmem_limit_bytes=24 << 20),
        name="front",
    )(slices, routes_t, weight_t, resid, cotangent, resid, cotangent)


def shifted(x, by):
    return pltpu.roll(x, x.shape[1] - by, 1)


def reverse_scan(factor, value):
    rows = factor.shape[1]
    lane = lax.broadcasted_iota(jnp.int32, factor.shape, 1)
    by = 1
    while by < rows:
        inside = lane < rows - by
        value = value + factor * jnp.where(inside, shifted(value, by), 0.0)
        factor = factor * jnp.where(inside, shifted(factor, by), 1.0)
        by *= 2
    return factor, value


MESH = pl.DeviceIdType.MESH


def place():
    sp, tp = lax.axis_index("sp"), lax.axis_index("tp")
    z, x, core = lax.div(sp, 4), lax.rem(sp, 4), lax.rem(tp, 2)
    right, left, across = lax.rem(tp + 2, 8), lax.rem(tp + 6, 8), lax.rem(tp + 4, 8)
    return sp, tp, z, x, right, left, across, 1 - 2 * core


def remote(src, dst, send, recv, sp, tp):
    return pltpu.make_async_remote_copy(
        src_ref=src, dst_ref=dst, send_sem=send, recv_sem=recv, device_id={"sp": sp, "tp": tp}, device_id_type=MESH
    )


def greet(peers):
    barrier = pltpu.get_barrier_semaphore()
    for sp, tp in peers:
        pl.semaphore_signal(barrier, inc=1, device_id={"sp": sp, "tp": tp}, device_id_type=MESH)
    return lambda: pl.semaphore_wait(barrier, len(peers))


def tail_kernel(back_ref, pick_ref, cot_t_ref, proj_ref, decay_ref, before_ref, states, gelu, slope, mixed,
                d_gate_ref, g_step_ref, g_log_ref, g_proj_ref,
                rg, term, from_x, sums, from_z, ends, ends_x, row, ends_z, dm, prod,
                ag_send, ag_l, ag_r, ag_a, ag_d, x_send, x_recv, z_send, z_recv, e_send, ex_recv, ez_recv):
    sp, tp, z, x, right, left, across, flip = place()
    mate = tp + flip
    channels, rows = decay_ref.shape
    depth = rg.shape[1]
    half_rows = depth // 2
    part = channels // 2
    xs = [z * 4 + lax.rem(x + d, 4) for d in range(1, 4)]
    zs = [lax.rem(z + d, 8) * 4 + x for d in range(1, 8)]
    arrive = greet([(sp, right), (sp, left), (sp, mate)] + [(q, tp) for q in xs + zs])

    slots = pick_ref.shape[0]
    routed = contract(back_ref[...].reshape(slots, depth), pick_ref[...], 0, 0)
    rg[tp] = (cot_t_ref[...].astype(F32) + routed).astype(BF16)
    arrive()

    def half(j, h):
        return rg.at[j, pl.ds(h * half_rows, half_rows), :]

    def moved(ref, k, recv, to):
        return remote(ref, ref, ag_send.at[k], recv, sp, to)

    sent = [
        moved(half(tp, 0), 0, ag_l.at[0], right),
        moved(half(tp, 1), 1, ag_r.at[1], left),
        moved(half(tp, 1), 2, ag_l.at[1], right),
        moved(half(tp, 0), 3, ag_r.at[0], left),
        moved(rg.at[tp], 4, ag_d.at[0], mate),
    ]
    for copy in sent:
        copy.start()

    def pass_on(ref, k, arrived, recv, to):
        moved(ref, k, arrived, to).wait_recv()
        copy = moved(ref, k, recv, to)
        copy.start()
        sent.append(copy)

    pass_on(half(left, 0), 5, ag_l.at[0], ag_a.at[0], right)
    pass_on(half(right, 1), 6, ag_r.at[1], ag_a.at[1], left)

    crossing = []

    def use(t, j):
        cols = pl.ds(pl.multiple_of(j * depth, depth), depth)
        piece = rg[j]
        term[j] = contract(piece, mixed[...], 1, 1).astype(BF16).reshape(term.shape[1:])
        for d in range(1, 4):
            to = lax.rem(x + d, 4)
            copy = remote(term.at[j, to], from_x.at[d - 1, j], x_send.at[t, d - 1], x_recv.at[t, d - 1], z * 4 + to, tp)
            copy.start()
            crossing.append(copy)
        product = contract(proj_ref[:, cols], piece, 1, 0)
        dm[...] = product if t == 0 else dm[...] + product

    use(0, tp)
    moved(rg.at[mate], 4, ag_d.at[0], mate).wait_recv()
    use(1, mate)
    moved(half(left, 1), 7, ag_l.at[1], mate).wait_recv()
    copy = moved(rg.at[left], 7, ag_d.at[1], mate)
    copy.start()
    sent.append(copy)
    moved(half(right, 0), 8, ag_r.at[0], mate).wait_recv()
    copy = moved(rg.at[right], 8, ag_d.at[2], mate)
    copy.start()
    sent.append(copy)
    use(2, left)
    use(3, right)
    pass_on(half(across, 0), 9, ag_a.at[0], ag_d.at[3], mate)
    pass_on(half(across, 1), 10, ag_a.at[1], ag_d.at[4], mate)
    moved(rg.at[left + flip], 7, ag_d.at[1], mate).wait_recv()
    use(4, left + flip)
    moved(rg.at[right + flip], 8, ag_d.at[2], mate).wait_recv()
    use(5, right + flip)
    use(6, across)
    moved(half(across + flip, 0), 9, ag_d.at[3], mate).wait_recv()
    moved(half(across + flip, 1), 10, ag_d.at[4], mate).wait_recv()
    use(7, across + flip)
    order = [tp, mate, left, right, left + flip, right + flip, across, across + flip]

    lines = [jnp.zeros((1, channels), F32), jnp.zeros((1, channels), F32)]
    for k in range(2):
        at = pl.ds(k * part, part)
        decays = jnp.exp(decay_ref[at, :])
        d_mixed = dm[at, :]
        d_gate_ref[at, :] = (d_mixed * states[at, :] * slope[at, :]).astype(BF16)
        lane = lax.broadcasted_iota(jnp.int32, decays.shape, 1)
        following = jnp.where(lane < rows - 1, shifted(decays, 1), 1.0)
        products, local = reverse_scan(following, d_mixed * gelu[at, :])
        prod[at, :] = products
        g_step_ref[at, :] = local
        same = lax.broadcasted_iota(jnp.int32, (part, channels), 0) + k * part == lax.broadcasted_iota(
            jnp.int32, (part, channels), 1
        )
        first = decays[:, 0:1]
        for i, ended in enumerate((products, local)):
            lines[i] = lines[i] + jnp.sum(jnp.where(same, first * ended[:, 0:1], 0.0), axis=0, keepdims=True)
    ends[...] = jnp.zeros_like(ends)
    row[...] = jnp.zeros_like(row)
    ends[0:1, :] = lines[0]
    ends[1:2, :] = lines[1]
    ends_x[x] = ends[...]
    passed = []
    for d in range(1, 4):
        copy = remote(ends, ends_x.at[x], e_send.at[d - 1], ex_recv.at[d - 1], z * 4 + lax.rem(x + d, 4), tp)
        copy.start()
        passed.append(copy)

    def cross_sum(t):
        j = order[t]
        total = term[j, x].astype(F32)
        for d in range(1, 4):
            remote(from_x.at[d - 1, j], from_x.at[d - 1, j], x_send.at[t, d - 1], x_recv.at[t, d - 1], sp, mate).wait_recv()
            total = total + from_x[d - 1, j].astype(F32)
        sums[j] = total.astype(BF16)

        @pl.when(j == z)
        def _():
            g_proj_ref[...] = total

        @pl.when(j != z)
        def _():
            remote(sums.at[j], from_z.at[z], z_send.at[j], z_recv.at[z], j * 4 + x, tp).start()

    for t in range(4):
        cross_sum(t)
    scale, shift = jnp.ones((1, channels), F32), jnp.zeros((1, channels), F32)
    for d in range(1, 4):
        q = lax.rem(x + 4 - d, 4)
        remote(ends, ends_x.at[q], e_send.at[d - 1], ex_recv.at[d - 1], sp, mate).wait_recv()
    for q in reversed(range(4)):
        shift = ends_x[q, 1:2, :] + ends_x[q, 0:1, :] * shift
        scale = ends_x[q, 0:1, :] * scale
    row[0:1, :] = scale
    row[1:2, :] = shift
    for d in range(1, 8):
        copy = remote(row, ends_z.at[z], e_send.at[d + 2], ez_recv.at[d - 1], lax.rem(z + d, 8) * 4 + x, tp)
        copy.start()
        passed.append(copy)
    for t in range(4, 8):
        cross_sum(t)
    for d in range(1, 8):
        q = lax.rem(z + 8 - d, 8)
        remote(row, ends_z.at[q], e_send.at[d + 2], ez_recv.at[d - 1], sp, mate).wait_recv()
    ends_z[z] = row[...]
    entering = jnp.zeros((1, channels), F32)
    for q in reversed(range(1, 8)):
        entering = jnp.where(q > z, ends_z[q, 1:2, :] + ends_z[q, 0:1, :] * entering, entering)
    for q in reversed(range(1, 4)):
        entering = jnp.where(q > x, ends_x[q, 1:2, :] + ends_x[q, 0:1, :] * entering, entering)
    for k in range(2):
        at = pl.ds(k * part, part)
        same = lax.broadcasted_iota(jnp.int32, (part, channels), 0) + k * part == lax.broadcasted_iota(
            jnp.int32, (part, channels), 1
        )
        column = jnp.sum(jnp.where(same, entering, 0.0), axis=1, keepdims=True)
        grad = g_step_ref[at, :] + prod[at, :] * column
        g_step_ref[at, :] = grad
        g_log_ref[at, :] = grad * jnp.exp(decay_ref[at, :]) * before_ref[at, :]
    for d in range(1, 8):
        q = lax.rem(z + d, 8)
        remote(from_z.at[q], from_z.at[q], z_send.at[q], z_recv.at[q], sp, mate).wait_recv()
        g_proj_ref[...] += from_z[q].astype(F32)
    for d in range(1, 8):
        q = lax.rem(z + d, 8)
        remote(sums.at[q], from_z.at[z], z_send.at[q], z_recv.at[z], sp, mate).wait_send()
    for copy in sent + crossing + passed:
        copy.wait_send()


def tail(back, pick, cot_t, proj, decay, before, states, gelu, slope, mixed):
    channels, rows = decay.shape
    depth = cot_t.shape[0]
    flat = (channels, rows)
    lines = 8 * depth // 32
    outs = [(flat, BF16), (flat, F32), (flat, F32), ((lines, channels), F32)]
    dma = pltpu.SemaphoreType.DMA
    return pl.pallas_call(
        tail_kernel,
        in_specs=[pl.BlockSpec(memory_space=VMEM)] * 10,
        out_specs=[pl.BlockSpec(memory_space=VMEM)] * 4,
        out_shape=[jax.ShapeDtypeStruct(s, d) for s, d in outs],
        scratch_shapes=[
            VMEM((8, depth, rows), BF16),
            VMEM((8, 4, lines, channels), BF16),
            VMEM((3, 8, lines, channels), BF16),
            VMEM((8, lines, channels), BF16),
            VMEM((8, lines, channels), BF16),
            VMEM((8, channels), F32),
            VMEM((4, 8, channels), F32),
            VMEM((8, channels), F32),
            VMEM((8, 8, channels), F32),
            VMEM(flat, F32),
            VMEM(flat, F32),
            dma((11,)), dma((2,)), dma((2,)), dma((2,)), dma((5,)),
            dma((8, 3)), dma((8, 3)), dma((8,)), dma((8,)), dma((10,)), dma((3,)), dma((7,)),
        ],
        compiler_params=pltpu.CompilerParams(collective_id=1, has_side_effects=True, vmem_limit_bytes=24 << 20),
        name="tail",
    )(back, pick, cot_t, proj, decay, before, states, gelu, slope, mixed)


N_SENDS = 14
ORDER = (0, 1, 7, 3, 5, 4, 2, 6)
FAR = (3, 6)


def experts_kernel(send_ref, w_gate_ref, w_up_ref, w_down_ref, gate_in, decay_in, before_in, step_in,
                   g_gate_ref, g_up_ref, g_down_ref, back_ref, states, gelu, slope, mixed,
                   gate_ref, decay_ref, before_ref, step_ref,
                   buf, w_cat, w_cat_t, w_down, w_down_t, acc_t, loads, parts, from_mate, pair, from_far, from_left, from_right, ret, back,
                   a_send, a_recv, far_send, far_recv, sends, yl, yr, ya, ym, pm, fa, fl, fr, b_send, b_recv):
    sp, tp, z, x, right, left, across, flip = place()
    mate = tp + flip
    core = lax.rem(tp, 2)
    y = lax.div(tp, 2)
    y_right, y_left, y_far = lax.rem(y + 1, 4), lax.rem(y + 3, 4), lax.rem(y + 2, 4)
    n_sp, both_caps, depth = send_ref.shape[1:]
    cap = both_caps // 2
    n_z = n_sp // 4
    steps = 2 * n_z
    arrive = greet([(lax.rem(sp + k, n_sp), tp) for k in range(1, n_sp)] + [(sp, right), (sp, left), (sp, mate)])

    def dz(i):
        found = 0
        for k, value in enumerate(ORDER):
            found = jnp.where(i == k, value, found)
        return found

    def source(i):
        return lax.rem(z + dz(i), n_z) * 4

    def target(i):
        return lax.rem(z - dz(i) + n_z, n_z) * 4

    def is_far(i):
        return (i >= FAR[0]) & (i < FAR[1])

    def out_copy(i, d):
        to = target(i) + lax.rem(x + d, 4)
        return remote(send_ref.at[0, to], buf.at[tp, sp], a_send.at[i, d], a_recv.at[i, x], to, tp)

    def out_far(i, d):
        to = target(i) + lax.rem(x + d, 4)
        return remote(send_ref.at[1, to], buf.at[across, sp], far_send.at[i, d], far_recv.at[i, x], to, tp)

    def back_copy(i, q):
        to = source(i) + q
        return remote(ret.at[to], back.at[sp], b_send.at[i, q], b_recv.at[i, x], to, tp)

    weights = [
        pltpu.make_async_copy(w_gate_ref, w_cat.at[:, 0:128], loads.at[0]),
        pltpu.make_async_copy(w_up_ref, w_cat.at[:, 128:256], loads.at[1]),
        pltpu.make_async_copy(w_down_ref, w_down, loads.at[2]),
        pltpu.make_async_copy(gate_in, gate_ref, loads.at[3]),
        pltpu.make_async_copy(decay_in, decay_ref, loads.at[4]),
        pltpu.make_async_copy(before_in, before_ref, loads.at[5]),
        pltpu.make_async_copy(step_in, step_ref, loads.at[6]),
    ]
    arrive()
    pltpu.make_async_copy(send_ref.at[0, sp], buf.at[tp, sp], a_recv.at[0, x]).start()
    pltpu.make_async_copy(send_ref.at[1, sp], buf.at[across, sp], far_recv.at[0, x]).start()
    for d in range(1, 4):
        out_copy(0, d).start()
        out_far(0, d).start()

    @pl.loop(1, n_z)
    def _(i):
        for d in range(4):
            out_copy(i, d).start()

        @pl.when(jnp.logical_not(is_far(i)))
        def _():
            for d in range(4):
                out_far(i, d).start()

    def wait(ref, sem):
        remote(ref, ref, a_send.at[0, 0], sem, sp, mate).wait_recv()

    for copy in weights:
        copy.start()

    def prepare(t):
        @pl.when(t == 0)
        def _():
            for copy in weights:
                copy.wait()
            acc_t[...] = jnp.zeros_like(acc_t)
            g_down_ref[...] = jnp.zeros_like(g_down_ref)

        for k in range(2):
            at = pl.ds(pl.multiple_of((2 * t + k) * depth, depth), depth)
            w_cat_t[:, at] = w_cat[at, :].astype(F32).T.astype(BF16)
            w_down_t[at, :] = w_down[:, at].astype(F32).T.astype(BF16)

    def activate(k):
        part = gate_ref.shape[0] // 2
        at = pl.ds(k * part, part)
        v = gate_ref[at, :].astype(F32)
        state = jnp.exp(decay_ref[at, :]) * before_ref[at, :] + step_ref[at, :].astype(F32)
        th = jnp.tanh(ROOT * (v + 0.044715 * (v * v * v)))
        act = 0.5 * v * (1.0 + th)
        gelu[at, :] = act
        states[at, :] = state
        slope[at, :] = 0.5 * (1.0 + th) + 0.5 * v * (1.0 - th * th) * (ROOT * (1.0 + 3.0 * 0.044715 * (v * v)))
        mixed[at, :] = (act * state).astype(BF16)

    def first(s):
        return source(lax.div(s, 2)) + 2 * lax.rem(s, 2)

    def far(s):
        return is_far(lax.div(s, 2))

    def sends_of(s, *which):
        at = first(s)
        blk = pl.ds(at, 2)

        def same(j, to, k, recv):
            return remote(buf.at[j, blk], buf.at[j, blk], sends.at[s, k], recv, sp, to)

        makers = [
            lambda: same(tp, right, 0, yl.at[s]),
            lambda: same(tp, left, 1, yr.at[s]),
            lambda: same(tp, mate, 2, ym.at[s, 0]),
            lambda: remote(buf.at[left, at], buf.at[left, at], sends.at[s, 3], ya.at[s, 0], sp, right),
            lambda: remote(buf.at[right, at + 1], buf.at[right, at + 1], sends.at[s, 4], ya.at[s, 1], sp, left),
            lambda: same(left, mate, 5, ym.at[s, 1]),
            lambda: same(right, mate, 6, ym.at[s, 2]),
            lambda: same(across, mate, 7, ym.at[s, 3]),
            lambda: remote(parts.at[1 - core, :, blk], from_mate.at[:, blk], sends.at[s, 8], pm.at[s], sp, mate),
            lambda: remote(pair.at[y_far, at], from_far.at[at], sends.at[s, 9], fa.at[s, 0], sp, right),
            lambda: remote(pair.at[y_far, at + 1], from_far.at[at + 1], sends.at[s, 10], fa.at[s, 1], sp, left),
            lambda: remote(pair.at[y_right, blk], from_left.at[blk], sends.at[s, 11], fl.at[s], sp, right),
            lambda: remote(pair.at[y_left, blk], from_right.at[blk], sends.at[s, 12], fr.at[s], sp, left),
        ]
        return [makers[k]() for k in which]

    def start(s, *which):
        for copy in sends_of(s, *which):
            copy.start()

    def spread(s):
        i, q = lax.div(s, 2), 2 * lax.rem(s, 2)
        at = first(s)
        for k in range(2):
            wait(buf.at[tp, at + k], a_recv.at[i, q + k])
        start(s, 0, 1, 2)

        @pl.when(jnp.logical_not(far(s)))
        def _():
            for k in range(2):
                wait(buf.at[across, at + k], far_recv.at[i, q + k])
            start(s, 7)

    def forward(s):
        blk = pl.ds(first(s), 2)
        wait(buf.at[left, blk], yl.at[s])
        wait(buf.at[right, blk], yr.at[s])

        @pl.when(far(s))
        def _():
            start(s, 3, 4)

        start(s, 5, 6)

    def hand_over(s):
        @pl.when(far(s))
        def _():
            wait(buf.at[across, first(s)], ya.at[s, 0])
            wait(buf.at[across, first(s) + 1], ya.at[s, 1])
            start(s, 7)

    def compute(s):
        blk = pl.ds(first(s), 2)
        for k, j in enumerate((tp, left, right, across)):
            wait(buf.at[j + flip, blk], ym.at[s, k])
        size = 2 * cap

        def rows_of(j):
            return buf[j, blk, 0:cap, :].reshape(size, depth)

        def cots_of(j):
            return buf[j, blk, cap : 2 * cap, :].reshape(size, depth)

        act = jnp.zeros((size, 256), F32)
        d_hidden = jnp.zeros((size, 128), F32)
        for j in range(8):
            cols = slice(j * depth, (j + 1) * depth)
            act = act + contract(rows_of(j), w_cat[cols, :], 1, 0)
            d_hidden = d_hidden + contract(cots_of(j), w_down_t[cols, :], 1, 0)
        gate_act, up_act = act[:, 0:128], act[:, 128:256]
        sig = jax.nn.sigmoid(gate_act)
        silu = gate_act * sig
        hidden = (silu * up_act).astype(BF16)
        d_gate = (d_hidden * up_act * (sig * (1.0 + gate_act * (1.0 - sig)))).astype(BF16)
        d_up = (d_hidden * silu).astype(BF16)
        d_both = jnp.concatenate([d_gate, d_up], axis=1)
        d_both_t = d_both.astype(F32).T.astype(BF16)
        hidden_t = hidden.astype(F32).T.astype(BF16)
        for j in range(8):
            cols = slice(j * depth, (j + 1) * depth)
            value = contract(d_both, w_cat_t[:, cols], 1, 0).astype(BF16)
            parts[j % 2, j // 2, blk] = value.reshape(2, cap, depth)
        start(s, 8)
        for j in range(8):
            cols = slice(j * depth, (j + 1) * depth)
            acc_t[:, cols] += contract(d_both_t, rows_of(j), 1, 0)
            g_down_ref[:, cols] += contract(hidden_t, cots_of(j), 1, 0)

    def pair_up(s):
        blk = pl.ds(first(s), 2)
        wait(from_mate.at[:, blk], pm.at[s])
        for k in range(4):
            pair[k, blk] = (parts[core, k, blk].astype(F32) + from_mate[k, blk].astype(F32)).astype(BF16)
        start(s, 9, 10)

    def join(s):
        at = first(s)
        for k, h in ((y_right, 0), (y_left, 1)):
            wait(from_far.at[at + h], fa.at[s, h])
            pair[k, at + h] = (pair[k, at + h].astype(F32) + from_far[at + h].astype(F32)).astype(BF16)
        start(s, 11, 12)

    def finish(s):
        i, q = lax.div(s, 2), 2 * lax.rem(s, 2)
        at = first(s)
        blk = pl.ds(at, 2)
        wait(from_left.at[blk], fl.at[s])
        wait(from_right.at[blk], fr.at[s])
        ret[blk] = (pair[y, blk].astype(F32) + from_left[blk].astype(F32) + from_right[blk].astype(F32)).astype(BF16)
        for k in range(2):
            @pl.when(at + k == sp)
            def _():
                pltpu.make_async_copy(ret.at[sp], back.at[sp], b_recv.at[0, x]).start()

            @pl.when(at + k != sp)
            def _():
                back_copy(i, q + k).start()

    stages = ((spread, 0), (forward, 2), (hand_over, 4), (finish, 10), (join, 8), (pair_up, 6), (compute, 5))

    @pl.loop(0, steps + 10)
    def _(t):
        for stage, late in stages:
            @pl.when((t >= late) & (t < steps + late))
            def _():
                stage(t - late)

        @pl.when(t < 4)
        def _():
            prepare(t)

        for k in range(2):
            @pl.when(t == 3 + k)
            def _():
                activate(k)

    for j in range(8):
        cols = slice(j * depth, (j + 1) * depth)
        both = acc_t[:, cols].T
        g_gate_ref[cols, :] = both[:, 0:128]
        g_up_ref[cols, :] = both[:, 128:256]

    @pl.loop(0, n_z)
    def _(i):
        for q in range(4):
            wait(back.at[target(i) + q], b_recv.at[i, q])

    back_ref[...] = back[...]

    @pl.loop(0, steps)
    def _(s):
        for copy in sends_of(s, 0, 1, 2, 5, 6, 7, 8, 9, 10, 11, 12):
            copy.wait_send()

        @pl.when(far(s))
        def _():
            for copy in sends_of(s, 3, 4):
                copy.wait_send()

    @pl.loop(0, n_z)
    def _(i):
        for d in range(4):
            @pl.when(target(i) + lax.rem(x + d, 4) != sp)
            def _():
                out_copy(i, d).wait_send()

                @pl.when(jnp.logical_not(is_far(i)))
                def _():
                    out_far(i, d).wait_send()

            @pl.when(source(i) + d != sp)
            def _():
                back_copy(i, d).wait_send()


def experts_pass(send, w_gate, w_up, w_down, gate, decay, before, step):
    _, n_sp, both_caps, depth = send.shape
    model, units = w_gate.shape
    cap = both_caps // 2
    block = (n_sp, cap, depth)
    n_z = n_sp // 4
    steps = 2 * n_z
    dma = pltpu.SemaphoreType.DMA
    outs = [((model, units), F32), ((model, units), F32), ((units, model), F32), (block, BF16)]
    flat = gate.shape
    outs += [(flat, F32), (flat, F32), (flat, F32), (flat, BF16)]
    return pl.pallas_call(
        experts_kernel,
        in_specs=[pl.BlockSpec(memory_space=pl.ANY)] * 8,
        out_specs=[pl.BlockSpec(memory_space=VMEM)] * 8,
        out_shape=[jax.ShapeDtypeStruct(s, d) for s, d in outs],
        scratch_shapes=[
            VMEM(flat, BF16),
            VMEM(flat, F32),
            VMEM(flat, F32),
            VMEM(flat, BF16),
            VMEM((8, n_sp, both_caps, depth), BF16),
            VMEM((model, 2 * units), BF16),
            VMEM((2 * units, model), BF16),
            VMEM((units, model), BF16),
            VMEM((model, units), BF16),
            VMEM((2 * units, model), F32),
            dma((7,)),
            VMEM((2, 4, *block), BF16),
            VMEM((4, *block), BF16),
            VMEM((4, *block), BF16),
            VMEM(block, BF16),
            VMEM(block, BF16),
            VMEM(block, BF16),
            VMEM(block, BF16),
            VMEM(block, BF16),
            dma((n_z, 4)), dma((n_z, 4)), dma((n_z, 4)), dma((n_z, 4)), dma((steps, N_SENDS)),
            dma((steps,)), dma((steps,)), dma((steps, 2)), dma((steps, 4)), dma((steps,)), dma((steps, 2)),
            dma((steps,)), dma((steps,)), dma((n_z, 4)), dma((n_z, 4)),
        ],
        compiler_params=pltpu.CompilerParams(collective_id=0, has_side_effects=True, vmem_limit_bytes=38 << 20),
        name="experts",
    )(send, w_gate, w_up, w_down, gate, decay, before, step)


def settle_kernel(*refs):
    n = len(refs) // 2
    copies = [pltpu.make_async_copy(refs[k], refs[n + k], refs[2 * n].at[k]) for k in range(n)]
    for copy in copies:
        copy.start()
    for copy in copies:
        copy.wait()


def settle(*values):
    return pl.pallas_call(
        settle_kernel,
        in_specs=[pl.BlockSpec(memory_space=VMEM)] * len(values),
        out_specs=[pl.BlockSpec(memory_space=pl.ANY)] * len(values),
        out_shape=[jax.ShapeDtypeStruct(a.shape, a.dtype) for a in values],
        scratch_shapes=[pltpu.SemaphoreType.DMA((len(values),))],
        compiler_params=pltpu.CompilerParams(vmem_limit_bytes=16 << 20),
        name="settle",
    )(*values)


def on_device(resid, cotangent, routes, route_weight, w_gate, w_up, w_down, out_proj, gate_pre, log_decay,
              state_before, step_input):
    rows, model = resid.shape
    experts, n_tp = lax.axis_size("sp"), lax.axis_size("tp")
    cap = 2 * rows * routes.shape[1] // experts
    send, pick, cot_t = front(routes.T, route_weight.T, resid, cotangent, experts, cap, n_tp)
    decay, before = log_decay.T, state_before.T
    done = experts_pass(send, w_gate[0], w_up[0], w_down[0], gate_pre.T, decay, before, step_input.T)
    ended = tail(done[3], pick, cot_t, out_proj.T, decay, before, *done[4:])
    grad_gate, grad_up, grad_down, d_gate, grad_step, grad_log, grad_proj = settle(*done[:3], *ended)
    return grad_gate[None], grad_up[None], grad_down[None], grad_proj, d_gate.T, grad_step.T, grad_log.T


def solution(mesh):
    by_sp, both = P("sp", None), P("sp", "tp")
    cols = P("sp", None, "tp")
    return jax.shard_map(
        on_device,
        mesh=mesh,
        in_specs=(by_sp, by_sp, by_sp, by_sp, cols, cols, P("sp", "tp", None), P(None, "tp"), both, both, both, both),
        out_specs=(cols, cols, P("sp", "tp", None), both, both, both, both),
        check_vma=False,
    )
```
